512 devices in a mesh: tp: 16 (over y, x), dp: 32 (over z, core).
Axes of the slice: x: 4, y: 4, z: 16, core: 2. Of those that a mesh axis runs over, the one named last changes fastest.
Arguments:
- hidden_vectors: bfloat16 [192, 4096], P('tp', 'dp'), may hold values from -8 to 8
- live_spans: int32 [96], P('dp'), may hold values from 1 to 2, as said below
- entry_rescale: bfloat16 [2, 4096], P(None, 'dp'), may hold values from 0.099609375 to 1.8984375
- query_weights: bfloat16 [2, 4096, 2048], P(None, 'dp', 'tp'), may hold values from -0.09375 to 0.09375
- address_weights: bfloat16 [2, 4096, 2048], P(None, 'dp', 'tp'), may hold values from -0.09375 to 0.09375
- content_weights: bfloat16 [2, 4096, 2048], P(None, 'dp', 'tp'), may hold values from -0.09375 to 0.09375
- fade_weights: bfloat16 [2, 4096, 2048], P(None, 'dp', 'tp'), may hold values from -0.09375 to 0.09375
- learning_speed_weights: bfloat16 [2, 4096, 2048], P(None, 'dp', 'tp'), may hold values from -0.09375 to 0.09375
- exit_valve_weights: bfloat16 [2, 4096, 2048], P(None, 'dp', 'tp'), may hold values from -0.09375 to 0.09375
- feature_fade_ceiling: float32 [2, 2048], P(None, 'tp'), may hold values from 0.02 to 2
- subspace_rescale: float32 [2, 2048], P(None, 'tp'), may hold values from 0.1 to 1.9
- exit_weights: bfloat16 [2, 2048, 4096], P(None, 'tp', 'dp'), may hold values from -0.125 to 0.125
- memories: float32 [2, 96, 32, 64, 64], P(None, 'dp', 'tp'), may hold values from -6 to 6
- extra_log_fade: float32 [2, 192, 32], P(None, 'dp', 'tp'), may hold values from -0.7 to 0
Outputs:
- hidden_out: bfloat16 [192, 4096], P('tp', 'dp')
- new_states: float32 [2, 96, 32, 64, 64], P(None, 'dp', 'tp')
The draws below stay inside these ranges and needn't reach their ends.
Inputs may be any that keep to these rules, and one draw needn't show every extreme that they name: `live_spans`: live slots of each sequence; some sequence has 2.
All inputs are finite; a program needn't handle non-finite values.
Results may differ from the reference program's by a relative error of at most 0.0075.
Values may be sent and summed in bfloat16 or wider, within the bound.
A program may use at most 64 MiB of HBM per device.

```python
import math
import jax
import jax.numpy as jnp
from jax import lax

D = 4096
HEADS = 32
HD = 64
WIDTH = 2048
STEPS = 2
SEQS = 96
TOKENS = 192


def draw_hidden_vectors(key, part):
    values = jnp.clip(jax.random.normal(key, (TOKENS, D), jnp.float32), -4.0, 4.0)
    ramp = 0.4 * 5.0 ** (jnp.arange(D, dtype=jnp.float32) / D)
    return (values * ramp[None, :]).astype(jnp.bfloat16)


def draw_live_spans(key, part):
    picker = jax.random.randint(jax.random.fold_in(key, 1), (SEQS,), 0, 4)
    longer = jax.random.randint(jax.random.fold_in(key, 2), (SEQS,), 2, STEPS + 1)
    result = jnp.where(picker == 0, longer, 1)
    return result.at[0].set(STEPS).astype(jnp.int32)


def draw_extra_log_fade(key, part):
    picker = jax.random.randint(jax.random.fold_in(key, 3), (2, TOKENS, HEADS), 0, 8)
    depth = jax.random.uniform(jax.random.fold_in(key, 4), (2, TOKENS, HEADS), jnp.float32, -0.7, -0.2)
    return jnp.where(picker == 0, depth, 0.0).astype(jnp.float32)


def block_levels(rng, extent, split, low, largest):
    factor_of, own = 1.0, jax.random.fold_in(rng, 6)
    for axis_at, shards_of in split:
        heights = jnp.exp(jax.random.uniform(jax.random.fold_in(own, axis_at), (shards_of,), jnp.float32, low / len(split), largest / len(split)))
        factor_of = factor_of * jnp.repeat(heights, extent[axis_at] // shards_of).reshape([-1 if axis == axis_at else 1 for axis in range(len(extent))])
    return factor_of


def scatter_about(stream_key, dims, deviation, limit, split=(), kind=jnp.bfloat16):
    values = jax.random.normal(stream_key, dims, jnp.float32) * deviation
    if len(split) > 0:
        values = block_levels(stream_key, dims, split, -0.22, 0.18) * values
    return jnp.clip(values, min=-limit, max=limit).astype(kind)


def setup_inputs(seed: int = 0) -> dict:
    arg_keys = jax.random.split(jax.random.key(seed), 15)
    hidden_vectors = draw_hidden_vectors(jax.random.fold_in(arg_keys[14], 71), 0)
    live_spans = draw_live_spans(jax.random.fold_in(arg_keys[14], 71), 0)
    entry_rescale = jnp.clip(1.0 + 0.18 * jax.random.normal(arg_keys[2], (2, D), jnp.float32), 0.099609375, 1.8984375).astype(jnp.bfloat16)
    query_weights = scatter_about(arg_keys[3], (2, D, WIDTH), D ** -0.5, 0.09375, ((1, 32), (2, 16)))
    address_weights = scatter_about(arg_keys[4], (2, D, WIDTH), D ** -0.5, 0.09375, ((1, 32), (2, 16)))
    content_weights = scatter_about(arg_keys[5], (2, D, WIDTH), D ** -0.5, 0.09375, ((1, 32), (2, 16)))
    fade_weights = scatter_about(arg_keys[6], (2, D, WIDTH), D ** -0.5, 0.09375, ((1, 32), (2, 16)))
    learning_speed_weights = scatter_about(arg_keys[7], (2, D, WIDTH), D ** -0.5, 0.09375, ((1, 32), (2, 16)))
    exit_valve_weights = scatter_about(arg_keys[8], (2, D, WIDTH), D ** -0.5, 0.09375, ((1, 32), (2, 16)))
    feature_fade_ceiling = jnp.clip(jnp.exp(math.log(2.0) - 4.6051702 * jax.random.uniform(arg_keys[9], (2, WIDTH), jnp.float32) ** block_levels(arg_keys[9], (2, WIDTH), ((1, 16),), -0.2, 0.2)), 0.02, 2.0)
    subspace_rescale = jnp.clip(1.0 + 0.18 * jax.random.normal(arg_keys[10], (2, WIDTH), jnp.float32), 0.1, 1.9)
    exit_weights = scatter_about(arg_keys[11], (2, WIDTH, D), WIDTH ** -0.5, 0.125, ((1, 16), (2, 32)))
    memories = scatter_about(arg_keys[12], (2, SEQS, HEADS, HD, HD), 1.0, 6.0, ((1, 32), (2, 16)), jnp.float32)
    extra_log_fade = draw_extra_log_fade(jax.random.fold_in(arg_keys[14], 71), 0)
    return dict(hidden_vectors=hidden_vectors, live_spans=live_spans, entry_rescale=entry_rescale, query_weights=query_weights, address_weights=address_weights, content_weights=content_weights, fade_weights=fade_weights, learning_speed_weights=learning_speed_weights, exit_valve_weights=exit_valve_weights, feature_fade_ceiling=feature_fade_ceiling, subspace_rescale=subspace_rescale, exit_weights=exit_weights, memories=memories, extra_log_fade=extra_log_fade)


NORM_EPS = 1e-06
GROUP_EPS = 0.00064

def memory_change(mapped_vectors, live_spans, feature_fade_ceiling, subspace_rescale, running_memory, extra_log_fade):
    batch_total, subspace_total, subspace_size = (running_memory.shape[0], running_memory.shape[1], running_memory.shape[2])
    position_total = mapped_vectors[0].shape[0] // batch_total

    def by_head(values):
        return values.reshape(batch_total, position_total, subspace_total, subspace_size)
    read_rows, key_rows, value_rows, fade_scores, rate_pre, gate_pre = [by_head(v) for v in mapped_vectors]
    fade_multiplier_lines = jnp.exp(extra_log_fade.reshape(batch_total, position_total, subspace_total, 1) - feature_fade_ceiling.reshape(subspace_total, subspace_size) * jax.nn.sigmoid(fade_scores))
    rate_rows = jax.nn.sigmoid(rate_pre)
    gate_rows = jax.nn.sigmoid(gate_pre)
    unit_keys = key_rows * lax.rsqrt(lax.optimization_barrier(jnp.sum(key_rows * key_rows, axis=3, keepdims=True)) + 1e-06)
    readouts = []
    for position in range(position_total):
        is_live = (live_spans > position).reshape(batch_total, 1, 1, 1)
        unit_now = unit_keys[:, position]
        removed = jnp.einsum('shvk,shk->shv', running_memory, -unit_now, precision=lax.Precision.HIGHEST)
        updated = running_memory * fade_multiplier_lines[:, position][:, :, None, :] + removed[..., None] * (unit_now * rate_rows[:, position])[:, :, None, :] + value_rows[:, position][..., None] * key_rows[:, position][:, :, None, :]
        running_memory = jnp.where(is_live, updated, running_memory)
        readouts.append(jnp.einsum('shvk,shk->shv', running_memory, read_rows[:, position], precision=lax.Precision.HIGHEST))
    readout = jnp.stack(readouts, axis=1)
    centered = readout - lax.optimization_barrier(jnp.mean(readout, axis=3, keepdims=True))
    normed = centered * lax.rsqrt(lax.optimization_barrier(jnp.mean(centered * centered, axis=3, keepdims=True)) + GROUP_EPS)
    normed = normed * subspace_rescale.reshape(subspace_total, subspace_size)
    live_rows = (jnp.arange(position_total)[None, :] < live_spans[:, None]).astype(jnp.float32)[:, :, None, None]
    blended_result = (normed * gate_rows * live_rows).astype(jnp.bfloat16)
    return (blended_result.reshape(batch_total * position_total, subspace_total * subspace_size), running_memory)

def reference(hidden_vectors, live_spans, entry_rescale, query_weights, address_weights, content_weights, fade_weights, learning_speed_weights, exit_valve_weights, feature_fade_ceiling, subspace_rescale, exit_weights, memories, extra_log_fade):
    rows_now = hidden_vectors
    new_states = []
    for layer_ordinal in range(2):
        float_rows = rows_now.astype(jnp.float32)
        row_scale = lax.rsqrt(lax.optimization_barrier(jnp.mean(float_rows * float_rows, axis=1)) + NORM_EPS)[:, None]
        gained = (float_rows * entry_rescale[layer_ordinal].astype(jnp.float32)).astype(jnp.bfloat16)
        mapped_vectors = tuple((jnp.dot(gained, weights[layer_ordinal], preferred_element_type=jnp.float32) * row_scale for weights in (query_weights, address_weights, content_weights, fade_weights, learning_speed_weights, exit_valve_weights)))
        blended_result, running_memory = memory_change(mapped_vectors, live_spans, feature_fade_ceiling[layer_ordinal], subspace_rescale[layer_ordinal], memories[layer_ordinal], extra_log_fade[layer_ordinal])
        mix_rows = jnp.dot(blended_result, exit_weights[layer_ordinal], preferred_element_type=jnp.float32)
        rows_now = (float_rows + mix_rows).astype(jnp.bfloat16)
        new_states.append(running_memory)
    return (rows_now, jnp.stack(new_states))
```

```python
import jax
import jax.numpy as jnp
from jax import lax
from jax.experimental import pallas as pl
from jax.experimental.pallas import tpu as pltpu
from jax.sharding import PartitionSpec as P

D = 4096
NORM_EPS = 1e-06
GROUP_EPS = 0.00064
TP = 16
NZ = 16
F32 = jnp.float32
BF16 = jnp.bfloat16
MESH = pl.DeviceIdType.MESH


def split_two(x):
    hi = x.astype(BF16)
    lo = (x - hi.astype(F32)).astype(BF16)
    return jnp.concatenate([hi, lo], axis=1)


def kernel(
    x_hbm, live_ref, gain_hbm, wq, wk, wv, wf, wl, we, ceil_hbm, resc_hbm, wo_hbm, mem_hbm, fade_hbm,
    out_hbm, st_hbm,
    xin, xrows, xs, xres, gains, wcat, wout, ceil, resc, fade, mem, packed, states,
    xg, acc, cs, cr, summed, ms, mg, gs, gr, xout,
    load_sem, wsend, wrecv, a_send, a_recv, c_send, c_recv, e_send, e_recv, g_send, g_recv, st_sem, out_sem,
):
    t = lax.axis_index("tp")
    d = lax.axis_index("dp")
    z = d // 2
    c = d % 2
    other = 1 - c

    barrier = pltpu.get_barrier_semaphore()

    def greet_plane(r, carry):
        to = (t + r) % TP
        pl.semaphore_signal(barrier, inc=1, device_id=(to, z * 2), device_id_type=MESH)
        pl.semaphore_signal(barrier, inc=1, device_id=(to, z * 2 + 1), device_id_type=MESH)
        return carry

    def greet_column(r, carry):
        to = (z + r) % NZ
        pl.semaphore_signal(barrier, inc=1, device_id=(t, to * 2 + c), device_id_type=MESH)
        return carry

    lax.fori_loop(1, NZ, greet_column, 0)
    lax.fori_loop(1, TP, greet_plane, 0)
    pl.semaphore_signal(barrier, inc=1, device_id=(t, z * 2 + other), device_id_type=MESH)

    mine = pl.ds(pl.multiple_of(c * 128, 128), 128)
    weights = (wq, wk, wv, wf, wl, we)
    loads = [pltpu.make_async_copy(x_hbm, xin, load_sem.at[0])]
    for p, w in enumerate(weights):
        loads.append(
            pltpu.make_async_copy(w, wcat.at[:, mine, pl.ds(p * 128, 128)], load_sem.at[1 + p])
        )
    loads.append(pltpu.make_async_copy(wo_hbm, wout.at[c], load_sem.at[7]))
    loads.append(pltpu.make_async_copy(gain_hbm, gains.at[c], load_sem.at[8]))
    loads.append(pltpu.make_async_copy(ceil_hbm, ceil, load_sem.at[9]))
    loads.append(pltpu.make_async_copy(resc_hbm, resc, load_sem.at[10]))
    loads.append(pltpu.make_async_copy(mem_hbm, mem, load_sem.at[11]))
    loads.append(pltpu.make_async_copy(fade_hbm, fade, load_sem.at[12]))
    for copy in loads:
        copy.start()

    lane = lax.broadcasted_iota(jnp.int32, (8, 128), 1)
    low_half = lane < 64
    row_at = lax.broadcasted_iota(jnp.int32, (256, 128), 0)
    lane_at = lax.broadcasted_iota(jnp.int32, (256, 128), 1)
    ones_block = jnp.where((row_at % 128) // 64 == lane_at // 64, 1.0, 0.0).astype(BF16)
    own_row = lax.broadcasted_iota(jnp.int32, (64, 128), 0)
    own_lane = lax.broadcasted_iota(jnp.int32, (64, 128), 1)
    diagonal = (own_lane % 64) == own_row

    def head_sum(x):
        return jnp.dot(split_two(x), ones_block, preferred_element_type=F32)

    loads[0].wait()
    xrows[...] = jnp.zeros((16, 128), F32)
    xrows[0:12, :] = xin[...].astype(F32)
    first = xrows[0:8, :]
    second = xrows[6:14, :]
    xres[0] = first
    xres[1] = second
    xs[0, 0] = first.astype(BF16)
    xs[0, 1] = second.astype(BF16)
    for copy in loads[1:]:
        copy.wait()

    pl.semaphore_wait(barrier, 2 * (TP - 1) + NZ)

    def plane_copy(b, to, core):
        return pltpu.make_async_remote_copy(
            src_ref=xs.at[b, core],
            dst_ref=xg.at[b, c * TP + t],
            send_sem=a_send.at[b],
            recv_sem=a_recv.at[b],
            device_id=(to, z * 2 + core),
            device_id_type=MESH,
        )

    def gather_plane(b):
        def step(r, carry):
            to = (t + r) % TP
            plane_copy(b, to, 0).start()
            plane_copy(b, to, 1).start()
            return carry

        lax.fori_loop(1, TP, step, 0)
        plane_copy(b, t, other).start()
        xg[b, c * TP + t] = xs[b, c]

    def swap(src, dst, i):
        return pltpu.make_async_remote_copy(
            src_ref=src,
            dst_ref=dst,
            send_sem=wsend.at[i],
            recv_sem=wrecv.at[i],
            device_id=(t, z * 2 + other),
            device_id_type=MESH,
        )

    gather_plane(0)
    theirs = wcat.at[:, mine, :]
    swaps = [
        swap(gains.at[c], gains.at[c], 0),
        swap(theirs, theirs, 1),
        swap(wout.at[c], wout.at[c], 2),
    ]
    for copy in swaps:
        copy.start()

    for b in range(2):
        for s in range(3):
            packed[b, s] = jnp.concatenate([mem[b, s, 0], mem[b, s, 1]], axis=1)

    def all_of(src, dst, send, recv):
        return pltpu.make_async_remote_copy(
            src_ref=src, dst_ref=dst, send_sem=send, recv_sem=recv,
            device_id=(t, z * 2 + other), device_id_type=MESH,
        )

    for b in range(2):
        if b == 0:
            for copy in swaps:
                copy.wait_recv()
        all_of(xg.at[b, 0:31], xg.at[b, 0:31], a_send.at[b], a_recv.at[b]).wait_recv()

        halves = [xg[b, h * TP : (h + 1) * TP].astype(F32).reshape(128, 128) for h in range(2)]
        gained = jnp.concatenate(
            [
                (halves[h] * gains[h, b : b + 1, :].astype(F32)).astype(BF16)
                for h in range(2)
            ],
            axis=1,
        )
        squares = jnp.sum(halves[0] * halves[0] + halves[1] * halves[1], axis=1, keepdims=True)
        squares = jnp.broadcast_to(squares, (128, 128)).reshape(TP, 8, 128)
        sixteen = lax.broadcasted_iota(jnp.int32, (TP, 3, 128), 2) < 64
        acc[:, 36:40, :] = jnp.zeros((TP, 4, 128), F32)
        acc[:, 36:39, :] = jnp.where(sixteen, squares[:, 0:3], squares[:, 3:6])
        for p in range(6):
            part = jnp.dot(
                gained, wcat[b, :, p * 128 : (p + 1) * 128], preferred_element_type=F32
            )
            acc[:, p * 6 : p * 6 + 6, :] = part.reshape(TP, 8, 128)[:, 0:6]
        cs[b] = acc[...].astype(BF16)

        def reduce_step(i, carry):
            away = (i + 1) // 2
            r = 8 + away * (2 * (i % 2) - 1)
            to = (z + r) % NZ
            pltpu.make_async_remote_copy(
                src_ref=cs.at[b, to],
                dst_ref=cr.at[b, z],
                send_sem=c_send.at[b],
                recv_sem=c_recv.at[b],
                device_id=(t, to * 2 + c),
                device_id_type=MESH,
            ).start()
            return carry

        lax.fori_loop(0, NZ - 1, reduce_step, 0)
        cr[b, z] = cs[b, z]

        row8 = lax.broadcasted_iota(jnp.int32, (8, 128), 0)
        live8 = jnp.zeros((8, 128), jnp.int32)
        for s in range(3):
            live8 = jnp.where(row8 // 2 == s, live_ref[s], live8)
        live_rows = (row8 % 2) < live8
        fade8 = jnp.where(low_half[0:6], fade[b, :, 0:1], fade[b, :, 1:2])

        all_of(cr.at[b, 0:15], cr.at[b, 0:15], c_send.at[b], c_recv.at[b]).wait_recv()
        summed[0:40, :] = jnp.sum(cr[b].astype(F32), axis=0)
        square_rows = summed[36:39, :]
        low_squares = square_rows[:, 0:1]
        high_squares = square_rows[:, 64:65]
        token_squares = jnp.concatenate([low_squares, high_squares], axis=0)
        row_scale = lax.rsqrt(token_squares / D + NORM_EPS)
        read, key, value, decay_pre, rate_pre, gate_pre = [
            summed[p * 6 : p * 6 + 6, :] * row_scale for p in range(6)
        ]
        decay = jnp.exp(fade8 - ceil[b : b + 1, :] * jax.nn.sigmoid(decay_pre))
        rate = jax.nn.sigmoid(rate_pre)
        gate = jax.nn.sigmoid(gate_pre)
        unit = key * lax.rsqrt(head_sum(key * key) + 1e-06)
        unit_rate = unit * rate
        spread = head_sum(
            jnp.concatenate(
                [jnp.where(diagonal, value[i : i + 1, :], 0.0) for i in range(6)], axis=0
            )
        )
        memory = [packed[b, s] for s in range(3)]
        readouts = [None] * 6
        for j in range(2):
            removed = head_sum(
                jnp.concatenate(
                    [memory[s] * unit[2 * s + j : 2 * s + j + 1, :] for s in range(3)], axis=0
                )
            )
            for s in range(3):
                i = 2 * s + j
                updated = (
                    memory[s] * decay[i : i + 1, :]
                    - removed[64 * s : 64 * s + 64] * unit_rate[i : i + 1, :]
                    + spread[64 * i : 64 * i + 64] * key[i : i + 1, :]
                )
                memory[s] = jnp.where(j < live_ref[s], updated, memory[s])
            read_out = head_sum(
                jnp.concatenate(
                    [memory[s] * read[2 * s + j : 2 * s + j + 1, :] for s in range(3)], axis=0
                )
            )
            for s in range(3):
                readouts[2 * s + j] = jnp.sum(
                    jnp.where(diagonal, read_out[64 * s : 64 * s + 64], 0.0), axis=0, keepdims=True
                )
        readout = jnp.concatenate(readouts, axis=0)
        centered = readout - head_sum(readout) * (1.0 / 64.0)
        variance = head_sum(centered * centered) * (1.0 / 64.0)
        normed = centered * lax.rsqrt(variance + GROUP_EPS) * resc[b : b + 1, :]
        mixed = jnp.where(live_rows[0:6], normed * gate, 0.0)
        ms[b] = jnp.concatenate([mixed, jnp.zeros((2, 128), F32)], axis=0).astype(BF16)

        def mixed_step(i, carry):
            away = (i + 1) // 2
            r = 8 + away * (2 * (i % 2) - 1)
            to = (z + r) % NZ
            pltpu.make_async_remote_copy(
                src_ref=ms.at[b],
                dst_ref=mg.at[b, z],
                send_sem=e_send.at[b],
                recv_sem=e_recv.at[b],
                device_id=(t, to * 2 + c),
                device_id_type=MESH,
            ).start()
            return carry

        lax.fori_loop(0, NZ - 1, mixed_step, 0)
        mg[b, z] = ms[b]
        for s in range(3):
            states[b, s, 0] = memory[s][:, 0:64]
            states[b, s, 1] = memory[s][:, 64:128]
        pltpu.make_async_copy(states.at[b], st_hbm.at[b], st_sem.at[b]).start()

        all_of(mg.at[b, 0:15], mg.at[b, 0:15], e_send.at[b], e_recv.at[b]).wait_recv()
        heads = mg[b].astype(F32).reshape(128, 128).astype(BF16)
        for h in range(2):
            part = jnp.dot(heads, wout[h, b], preferred_element_type=F32)
            gs[b, h] = part.reshape(NZ, 8, 128).astype(BF16)

        def owner_copy(to, core):
            return pltpu.make_async_remote_copy(
                src_ref=gs.at[b, core, to],
                dst_ref=gr.at[b, c * TP + t],
                send_sem=g_send.at[b],
                recv_sem=g_recv.at[b],
                device_id=(to, z * 2 + core),
                device_id_type=MESH,
            )

        def owner_step(r, carry):
            to = (t + r) % TP
            owner_copy(to, 0).start()
            owner_copy(to, 1).start()
            return carry

        lax.fori_loop(1, TP, owner_step, 0)
        owner_copy(t, other).start()
        gr[b, c * TP + t] = gs[b, c, t]

        all_of(gr.at[b, 0:31], gr.at[b, 0:31], g_send.at[b], g_recv.at[b]).wait_recv()
        for h in range(2):
            mix = jnp.sum(gr[b, h * TP : (h + 1) * TP].astype(F32), axis=0)
            following = (xres[h] + mix).astype(BF16)
            if b == 0:
                xs[1, h] = following
                xres[h] = following.astype(F32)
            else:
                xrows[6 * h : 6 * h + 6, :] = following.astype(F32)[0:6]
        if b == 0:
            gather_plane(1)
        else:
            xout[...] = xrows[0:12, :].astype(BF16)
            final = pltpu.make_async_copy(xout, out_hbm, out_sem)
            final.start()

    for copy in swaps:
        copy.wait_send()
    for b in range(2):
        pltpu.make_async_copy(states.at[b], st_hbm.at[b], st_sem.at[b]).wait()
        all_of(xg.at[b, 0:31], xg.at[b, 0:31], a_send.at[b], a_recv.at[b]).wait_send()
        all_of(cr.at[b, 0:15], cr.at[b, 0:15], c_send.at[b], c_recv.at[b]).wait_send()
        all_of(mg.at[b, 0:15], mg.at[b, 0:15], e_send.at[b], e_recv.at[b]).wait_send()
        all_of(gr.at[b, 0:31], gr.at[b, 0:31], g_send.at[b], g_recv.at[b]).wait_send()
    final.wait()


def shards(*arrays):
    hbm = pl.BlockSpec(memory_space=pltpu.HBM)
    in_specs = [hbm] * 14
    in_specs[1] = pl.BlockSpec(memory_space=pltpu.SMEM)
    dma = pltpu.SemaphoreType.DMA
    return pl.pallas_call(
        kernel,
        out_shape=(
            jax.ShapeDtypeStruct((12, 128), BF16),
            jax.ShapeDtypeStruct((2, 3, 2, 64, 64), F32),
        ),
        in_specs=in_specs,
        out_specs=(hbm, hbm),
        scratch_shapes=[
            pltpu.VMEM((12, 128), BF16),
            pltpu.VMEM((16, 128), F32),
            pltpu.VMEM((2, 2, 8, 128), BF16),
            pltpu.VMEM((2, 8, 128), F32),
            pltpu.VMEM((2, 2, 128), BF16),
            pltpu.VMEM((2, 256, 768), BF16),
            pltpu.VMEM((2, 2, 128, 128), BF16),
            pltpu.VMEM((2, 128), F32),
            pltpu.VMEM((2, 128), F32),
            pltpu.VMEM((2, 6, 2), F32),
            pltpu.VMEM((2, 3, 2, 64, 64), F32),
            pltpu.VMEM((2, 3, 64, 128), F32),
            pltpu.VMEM((2, 3, 2, 64, 64), F32),
            pltpu.VMEM((2, 32, 8, 128), BF16),
            pltpu.VMEM((16, 40, 128), F32),
            pltpu.VMEM((2, 16, 40, 128), BF16),
            pltpu.VMEM((2, 16, 40, 128), BF16),
            pltpu.VMEM((40, 128), F32),
            pltpu.VMEM((2, 8, 128), BF16),
            pltpu.VMEM((2, 16, 8, 128), BF16),
            pltpu.VMEM((2, 2, 16, 8, 128), BF16),
            pltpu.VMEM((2, 32, 8, 128), BF16),
            pltpu.VMEM((12, 128), BF16),
            dma((13,)),
            dma((3,)),
            dma((3,)),
            dma((2,)),
            dma((2,)),
            dma((2,)),
            dma((2,)),
            dma((2,)),
            dma((2,)),
            dma((2,)),
            dma((2,)),
            dma((2,)),
            dma,
        ],
        compiler_params=pltpu.CompilerParams(collective_id=0, has_side_effects=True),
    )(*arrays)


def solution(mesh):
    in_specs = (
        P("tp", "dp"),
        P("dp"),
        P(None, "dp"),
        P(None, "dp", "tp"),
        P(None, "dp", "tp"),
        P(None, "dp", "tp"),
        P(None, "dp", "tp"),
        P(None, "dp", "tp"),
        P(None, "dp", "tp"),
        P(None, "tp"),
        P(None, "tp"),
        P(None, "tp", "dp"),
        P(None, "dp", "tp", None, None),
        P(None, "dp", "tp"),
    )
    out_specs = (P("tp", "dp"), P(None, "dp", "tp", None, None))
    return jax.shard_map(shards, mesh=mesh, in_specs=in_specs, out_specs=out_specs, check_vma=False)
```

```python
import jax
import jax.numpy as jnp
from jax import lax
from jax.experimental import pallas as pl
from jax.experimental.pallas import tpu as pltpu
from jax.sharding import PartitionSpec as P

D = 4096
NORM_EPS = 1e-06
GROUP_EPS = 0.00064
TP = 16
NZ = 16
WIDTH = 2048
F32 = jnp.float32
BF16 = jnp.bfloat16
MESH = pl.DeviceIdType.MESH


def split_two(x):
    hi = x.astype(BF16)
    lo = (x - hi.astype(F32)).astype(BF16)
    return jnp.concatenate([hi, lo], axis=1)


def kernel(
    x_hbm, live_ref, gain_hbm, wq, wk, wv, wf, wl, we, ceil_hbm, resc_hbm, wo_hbm, mem_hbm, fade_hbm,
    out_hbm, st_hbm,
    xin, xrows, xs, gains, wcat, wall0, wall1, ceil, resc, fade, mem, packed, states,
    xg, acc, cs, cr, summed, ms, mg, xw, x1s, xr1, fin, xout,
    load_sem, swap_send, swap_recv, a_send, a_recv, c_send, c_recv, e_send, e_recv, f_send, f_recv,
    w_send, w_recv, l_send, l_recv, st_sem, out_sem,
):
    t = lax.axis_index("tp")
    d = lax.axis_index("dp")
    z = d // 2
    c = d % 2
    other = 1 - c
    away = (t + NZ - z) % NZ
    past_half = away // 9
    slot_here = (1 - past_half) * (2 * away - (away + 15) // 16) + past_half * (32 - 2 * away)

    barrier = pltpu.get_barrier_semaphore()

    def greet_plane(r, carry):
        to = (t + r) % TP
        pl.semaphore_signal(barrier, inc=1, device_id=(to, z * 2), device_id_type=MESH)
        pl.semaphore_signal(barrier, inc=1, device_id=(to, z * 2 + 1), device_id_type=MESH)
        return carry

    def greet_column(r, carry):
        to = (z + r) % NZ
        pl.semaphore_signal(barrier, inc=1, device_id=(t, to * 2 + c), device_id_type=MESH)
        return carry

    lax.fori_loop(1, NZ, greet_column, 0)
    lax.fori_loop(1, TP, greet_plane, 0)
    pl.semaphore_signal(barrier, inc=1, device_id=(t, z * 2 + other), device_id_type=MESH)

    mine = pl.ds(pl.multiple_of(c * 128, 128), 128)
    weights = (wq, wk, wv, wf, wl, we)
    loads = [pltpu.make_async_copy(x_hbm, xin, load_sem.at[0])]
    for p, w in enumerate(weights):
        loads.append(
            pltpu.make_async_copy(w, wcat.at[:, mine, pl.ds(p * 128, 128)], load_sem.at[1 + p])
        )
    loads.append(pltpu.make_async_copy(wo_hbm.at[0], wall0.at[t, :, mine], load_sem.at[7]))
    loads.append(pltpu.make_async_copy(wo_hbm.at[1], wall1.at[t], load_sem.at[13]))
    loads.append(pltpu.make_async_copy(gain_hbm, gains.at[c], load_sem.at[8]))
    loads.append(pltpu.make_async_copy(ceil_hbm, ceil, load_sem.at[9]))
    loads.append(pltpu.make_async_copy(resc_hbm, resc, load_sem.at[10]))
    loads.append(pltpu.make_async_copy(mem_hbm, mem, load_sem.at[11]))
    loads.append(pltpu.make_async_copy(fade_hbm, fade, load_sem.at[12]))
    for copy in loads:
        copy.start()

    lane = lax.broadcasted_iota(jnp.int32, (8, 128), 1)
    low_half = lane < 64
    row_at = lax.broadcasted_iota(jnp.int32, (256, 128), 0)
    lane_at = lax.broadcasted_iota(jnp.int32, (256, 128), 1)
    ones_block = jnp.where((row_at % 128) // 64 == lane_at // 64, 1.0, 0.0).astype(BF16)
    own_row = lax.broadcasted_iota(jnp.int32, (64, 128), 0)
    own_lane = lax.broadcasted_iota(jnp.int32, (64, 128), 1)
    diagonal = (own_lane % 64) == own_row

    def head_sum(x):
        return jnp.dot(split_two(x), ones_block, preferred_element_type=F32)

    loads[0].wait()
    xrows[...] = jnp.zeros((16, 128), F32)
    xrows[0:12, :] = xin[...].astype(F32)
    first = xrows[0:8, :]
    second = xrows[6:14, :]
    xs[0] = first.astype(BF16)
    xs[1] = second.astype(BF16)
    for copy in loads[1:]:
        copy.wait()

    pl.semaphore_wait(barrier, 2 * (TP - 1) + NZ)

    def remote(src, dst, send, recv, to_t, to_z, to_c):
        return pltpu.make_async_remote_copy(
            src_ref=src, dst_ref=dst, send_sem=send, recv_sem=recv,
            device_id=(to_t, to_z * 2 + to_c), device_id_type=MESH,
        )

    def to_sibling(src, i):
        return remote(src, src, swap_send.at[i], swap_recv.at[i], t, z, other)

    def row_copy(to, core):
        return remote(
            xs.at[core], xg.at[c, slot_here], a_send, a_recv, to, z, core
        )

    def row_step(r, carry):
        to = (t + r) % TP
        row_copy(to, 0).start()
        row_copy(to, 1).start()
        return carry

    lax.fori_loop(1, TP, row_step, 0)
    row_copy(t, other).start()
    xg[c, slot_here] = xs[c]

    swaps = [
        to_sibling(gains.at[c], 0),
        to_sibling(wcat.at[0, mine, :], 1),
        to_sibling(wcat.at[1, mine, :], 2),
        to_sibling(wall0.at[:, :, mine], 3),
    ]
    swaps[0].start()
    swaps[1].start()

    def exit_step(r, carry):
        mine_here = wall0.at[t, :, mine]
        remote(mine_here, mine_here, w_send.at[0], w_recv.at[0], (t + r) % TP, z, c).start()
        return carry

    lax.fori_loop(1, TP, exit_step, 0)

    def exit_step_last(r, carry):
        remote(wall1.at[t], wall1.at[t], w_send.at[1], w_recv.at[1], (t + r) % TP, z, c).start()
        return carry

    for b in range(2):
        for s in range(3):
            packed[b, s] = jnp.concatenate([mem[b, s, 0], mem[b, s, 1]], axis=1)

    fade_columns = jnp.transpose(jnp.concatenate([fade[0], fade[1], jnp.zeros((4, 6), F32)], axis=0))

    def all_of(ref, send, recv):
        return remote(ref, ref, send, recv, t, z, other)

    def column(start, first, last):
        if last == 8:
            start((z + 8) % NZ, 15, 15)

        def step(i, carry):
            dist = min(last, 7) - i
            start((z + dist) % NZ, 2 * dist - 1, 2 * dist)
            start((z + NZ - dist) % NZ, 2 * dist, 2 * dist - 1)
            return carry

        lax.fori_loop(0, min(last, 7) - first + 1, step, 0)

    def project(b, rows, lo, hi):
        count = (hi - lo) * 8
        gained = jnp.concatenate(
            [(rows[h] * gains[h, b : b + 1, :].astype(F32)).astype(BF16) for h in range(2)],
            axis=1,
        )
        squares = jnp.sum(rows[0] * rows[0] + rows[1] * rows[1], axis=1, keepdims=True)
        squares = jnp.broadcast_to(squares, (count, 128)).reshape(hi - lo, 8, 128)
        lower = lax.broadcasted_iota(jnp.int32, (hi - lo, 3, 128), 2) < 64
        acc[lo:hi, 36:40, :] = jnp.zeros((hi - lo, 4, 128), F32)
        acc[lo:hi, 36:39, :] = jnp.where(lower, squares[:, 0:3], squares[:, 3:6])
        for p in range(6):
            part = jnp.dot(
                gained, wcat[b, :, p * 128 : (p + 1) * 128], preferred_element_type=F32
            )
            acc[lo:hi, p * 6 : p * 6 + 6, :] = part.reshape(hi - lo, 8, 128)[:, 0:6]
        cs[b, lo:hi] = acc[lo:hi].astype(BF16)

    def send_partials(b, first, last):
        def start(to, here, there):
            remote(cs.at[b, here], cr.at[b, z], c_send.at[b], c_recv.at[b], t, to, c).start()

        column(start, first, last)

    groups = ((0, 7, 1, 3), (7, 13, 4, 6), (13, 16, 7, 8))
    for b in range(2):
        if b == 0:
            swaps[0].wait_recv()
            swaps[1].wait_recv()
            all_of(fin.at[0:31], a_send, a_recv).wait_recv()
            rows = [xg[h].astype(F32).reshape(128, 128) for h in range(2)]
            project(0, rows, 0, 16)
            send_partials(0, 1, 8)
            lax.fori_loop(1, TP, exit_step_last, 0)
        else:
            swaps[2].wait_recv()
            swaps[3].wait_recv()
            for g, (lo, hi, first, last) in enumerate(groups):
                count = (hi - lo) * 8
                all_of(xw.at[0:15, lo:hi], f_send.at[g], f_recv.at[g]).wait_recv()
                heads = jnp.concatenate(
                    [xw[i, lo:hi].astype(F32).reshape(count, 128).astype(BF16) for i in range(TP)],
                    axis=1,
                )
                mix = jnp.dot(
                    heads, wall0[...].reshape(WIDTH, 256), preferred_element_type=F32
                )
                rows = []
                for h in range(2):
                    before = xg[h, lo:hi].astype(F32).reshape(count, 128)
                    after = (before + mix[:, 128 * h : 128 * h + 128]).astype(BF16).astype(F32)
                    x1s[h, lo:hi] = after.reshape(hi - lo, 8, 128).astype(BF16)
                    rows.append(after)
                project(1, rows, lo, hi)
                send_partials(1, first, last)
            residual = remote(
                x1s.at[other, slot_here], xr1, l_send, l_recv, t, z, other
            )
            residual.start()
        own = cs[b, 0]
        cr[b, z] = own

        row8 = lax.broadcasted_iota(jnp.int32, (8, 128), 0)
        live8 = jnp.zeros((8, 128), jnp.int32)
        for s in range(3):
            live8 = jnp.where(row8 // 2 == s, live_ref[s], live8)
        live_rows = (row8 % 2) < live8
        fade8 = jnp.where(low_half[0:6], fade_columns[:, 2 * b : 2 * b + 1], fade_columns[:, 2 * b + 1 : 2 * b + 2])

        all_of(cr.at[b, 0:15], c_send.at[b], c_recv.at[b]).wait_recv()
        summed[0:40, :] = jnp.sum(cr[b].astype(F32), axis=0)
        square_rows = summed[36:39, :]
        low_squares = square_rows[:, 0:1]
        high_squares = square_rows[:, 64:65]
        token_squares = jnp.concatenate([low_squares, high_squares], axis=0)
        row_scale = lax.rsqrt(token_squares / D + NORM_EPS)
        read, key, value, decay_pre, rate_pre, gate_pre = [
            summed[p * 6 : p * 6 + 6, :] * row_scale for p in range(6)
        ]
        decay = jnp.exp(fade8 - ceil[b : b + 1, :] * jax.nn.sigmoid(decay_pre))
        rate = jax.nn.sigmoid(rate_pre)
        gate = jax.nn.sigmoid(gate_pre)
        unit = key * lax.rsqrt(head_sum(key * key) + 1e-06)
        unit_rate = unit * rate
        spread = head_sum(
            jnp.concatenate(
                [jnp.where(diagonal, value[i : i + 1, :], 0.0) for i in range(6)], axis=0
            )
        )
        memory = [packed[b, s] for s in range(3)]
        readouts = [None] * 6
        for j in range(2):
            removed = head_sum(
                jnp.concatenate(
                    [memory[s] * unit[2 * s + j : 2 * s + j + 1, :] for s in range(3)], axis=0
                )
            )
            for s in range(3):
                i = 2 * s + j
                updated = (
                    memory[s] * decay[i : i + 1, :]
                    - removed[64 * s : 64 * s + 64] * unit_rate[i : i + 1, :]
                    + spread[64 * i : 64 * i + 64] * key[i : i + 1, :]
                )
                memory[s] = jnp.where(j < live_ref[s], updated, memory[s])
            read_out = head_sum(
                jnp.concatenate(
                    [memory[s] * read[2 * s + j : 2 * s + j + 1, :] for s in range(3)], axis=0
                )
            )
            for s in range(3):
                readouts[2 * s + j] = jnp.sum(
                    jnp.where(diagonal, read_out[64 * s : 64 * s + 64], 0.0), axis=0, keepdims=True
                )
        readout = jnp.concatenate(readouts, axis=0)
        centered = readout - head_sum(readout) * (1.0 / 64.0)
        variance = head_sum(centered * centered) * (1.0 / 64.0)
        normed = centered * lax.rsqrt(variance + GROUP_EPS) * resc[b : b + 1, :]
        mixed = jnp.where(live_rows[0:6], normed * gate, 0.0)
        ms[b] = jnp.concatenate([mixed, jnp.zeros((2, 128), F32)], axis=0).astype(BF16)

        if b == 0:
            for g in (2, 1, 0):
                lo, hi, first, last = groups[g]

                def start(to, here, there):
                    remote(
                        ms.at[0], mg.at[there], e_send.at[g], e_recv.at[g], t, to, c
                    ).start()

                column(start, first, last)
            mg[0] = ms[0]
            all_of(wall0.at[0:15, :, mine], w_send.at[0], w_recv.at[0]).wait_recv()
            swaps[3].start()
            swaps[2].start()
        else:
            def start_both(to, here, there):
                for core in range(2):
                    remote(
                        ms.at[1], fin.at[c * TP + t], e_send.at[3], e_recv.at[3], z, to, core
                    ).start()

            column(start_both, 1, 8)

            @pl.when(t == z)
            def _():
                remote(
                    ms.at[1], fin.at[c * TP + t], e_send.at[3], e_recv.at[3], z, z, other
                ).start()
                fin[c * TP + t] = ms[1]

            @pl.when(t != z)
            def _():
                for core in range(2):
                    remote(
                        ms.at[1], fin.at[c * TP + t], e_send.at[3], e_recv.at[3], z, z, core
                    ).start()

        for s in range(3):
            states[b, s, 0] = memory[s][:, 0:64]
            states[b, s, 1] = memory[s][:, 64:128]
        pltpu.make_async_copy(states.at[b], st_hbm.at[b], st_sem.at[b]).start()

        if b == 0:
            for g, (lo, hi, first, last) in enumerate(groups):
                arriving = mg.at[max(lo, 1) : hi]
                all_of(arriving, e_send.at[g], e_recv.at[g]).wait_recv()

                def forward(r, carry):
                    remote(
                        mg.at[lo:hi], xw.at[t, lo:hi], f_send.at[g], f_recv.at[g],
                        (t + r) % TP, z, c,
                    ).start()
                    return carry

                lax.fori_loop(1, TP, forward, 0)
                xw[t, lo:hi] = mg[lo:hi]

    all_of(wall1.at[0:15], w_send.at[1], w_recv.at[1]).wait_recv()
    residual.wait_recv()

    @pl.when(t == z)
    def _():
        all_of(fin.at[0:31], e_send.at[3], e_recv.at[3]).wait_recv()

    @pl.when(t != z)
    def _():
        all_of(fin, e_send.at[3], e_recv.at[3]).wait_recv()

    heads = jnp.concatenate(
        [
            jnp.concatenate([fin[i].astype(F32), fin[TP + i].astype(F32)], axis=0).astype(BF16)
            for i in range(TP)
        ],
        axis=1,
    )
    mix = jnp.dot(heads, wall1[...].reshape(WIDTH, 128), preferred_element_type=F32)
    here_rows = x1s[c, slot_here].astype(F32)
    there_rows = xr1[...].astype(F32)
    core = jnp.full((8, 128), c, jnp.int32)
    xrows[0:6, :] = (jnp.where(core == 0, here_rows, there_rows) + mix[0:8])[0:6]
    xrows[6:12, :] = (jnp.where(core == 0, there_rows, here_rows) + mix[8:16])[0:6]
    xout[...] = xrows[0:12, :].astype(BF16)
    final = pltpu.make_async_copy(xout, out_hbm, out_sem)
    final.start()

    for copy in swaps:
        copy.wait_send()
    residual.wait_send()
    all_of(fin.at[0:31], a_send, a_recv).wait_send()
    all_of(wall0.at[0:15, :, mine], w_send.at[0], w_recv.at[0]).wait_send()
    all_of(wall1.at[0:15], w_send.at[1], w_recv.at[1]).wait_send()
    for b in range(2):
        pltpu.make_async_copy(states.at[b], st_hbm.at[b], st_sem.at[b]).wait()
        all_of(cr.at[b, 0:15], c_send.at[b], c_recv.at[b]).wait_send()
    for g, (lo, hi, first, last) in enumerate(groups):
        all_of(mg.at[max(lo, 1) : hi], e_send.at[g], e_recv.at[g]).wait_send()
        all_of(xw.at[0:15, lo:hi], f_send.at[g], f_recv.at[g]).wait_send()

    @pl.when(t == z)
    def _():
        all_of(fin.at[0:31], e_send.at[3], e_recv.at[3]).wait_send()

    @pl.when(t != z)
    def _():
        all_of(fin, e_send.at[3], e_recv.at[3]).wait_send()

    final.wait()


def shards(*arrays):
    arrays = arrays[:13] + (jnp.transpose(arrays[13], (0, 2, 1)),)
    hbm = pl.BlockSpec(memory_space=pltpu.HBM)
    in_specs = [hbm] * 14
    in_specs[1] = pl.BlockSpec(memory_space=pltpu.SMEM)
    dma = pltpu.SemaphoreType.DMA
    return pl.pallas_call(
        kernel,
        out_shape=(
            jax.ShapeDtypeStruct((12, 128), BF16),
            jax.ShapeDtypeStruct((2, 3, 2, 64, 64), F32),
        ),
        in_specs=in_specs,
        out_specs=(hbm, hbm),
        scratch_shapes=[
            pltpu.VMEM((12, 128), BF16),
            pltpu.VMEM((16, 128), F32),
            pltpu.VMEM((2, 8, 128), BF16),
            pltpu.VMEM((2, 2, 128), BF16),
            pltpu.VMEM((2, 256, 768), BF16),
            pltpu.VMEM((16, 128, 256), BF16),
            pltpu.VMEM((16, 128, 128), BF16),
            pltpu.VMEM((2, 128), F32),
            pltpu.VMEM((2, 128), F32),
            pltpu.VMEM((2, 2, 6), F32),
            pltpu.VMEM((2, 3, 2, 64, 64), F32),
            pltpu.VMEM((2, 3, 64, 128), F32),
            pltpu.VMEM((2, 3, 2, 64, 64), F32),
            pltpu.VMEM((2, 16, 8, 128), BF16),
            pltpu.VMEM((16, 40, 128), F32),
            pltpu.VMEM((2, 16, 40, 128), BF16),
            pltpu.VMEM((2, 16, 40, 128), BF16),
            pltpu.VMEM((40, 128), F32),
            pltpu.VMEM((2, 8, 128), BF16),
            pltpu.VMEM((16, 8, 128), BF16),
            pltpu.VMEM((16, 16, 8, 128), BF16),
            pltpu.VMEM((2, 16, 8, 128), BF16),
            pltpu.VMEM((8, 128), BF16),
            pltpu.VMEM((32, 8, 128), BF16),
            pltpu.VMEM((12, 128), BF16),
            dma((14,)),
            dma((4,)),
            dma((4,)),
            dma,
            dma,
            dma((2,)),
            dma((2,)),
            dma((4,)),
            dma((4,)),
            dma((3,)),
            dma((3,)),
            dma((2,)),
            dma((2,)),
            dma,
            dma,
            dma((2,)),
            dma,
        ],
        compiler_params=pltpu.CompilerParams(collective_id=0, has_side_effects=True),
    )(*arrays)


def solution(mesh):
    in_specs = (
        P("tp", "dp"),
        P("dp"),
        P(None, "dp"),
        P(None, "dp", "tp"),
        P(None, "dp", "tp"),
        P(None, "dp", "tp"),
        P(None, "dp", "tp"),
        P(None, "dp", "tp"),
        P(None, "dp", "tp"),
        P(None, "tp"),
        P(None, "tp"),
        P(None, "tp", "dp"),
        P(None, "dp", "tp", None, None),
        P(None, "dp", "tp"),
    )
    out_specs = (P("tp", "dp"), P(None, "dp", "tp", None, None))
    return jax.shard_map(shards, mesh=mesh, in_specs=in_specs, out_specs=out_specs, check_vma=False)
```

```python
import jax
import jax.numpy as jnp
from jax import lax
from jax.experimental import pallas as pl
from jax.experimental.pallas import tpu as pltpu
from jax.sharding import PartitionSpec as P

D = 4096
NORM_EPS = 1e-06
GROUP_EPS = 0.00064
TP = 16
NZ = 16
NEAR = 4
WIDTH = 2048
F32 = jnp.float32
BF16 = jnp.bfloat16
MESH = pl.DeviceIdType.MESH


def split_two(x):
    hi = x.astype(BF16)
    lo = (x - hi.astype(F32)).astype(BF16)
    return jnp.concatenate([hi, lo], axis=1)


def kernel(
    x_hbm, live_hbm, gain_hbm, wq, wk, wv, wf, wl, we, ceil_hbm, resc_hbm, wo_hbm, mem_hbm, fade_hbm,
    out_ref, states,
    live_ref, xin, xrows, xs, gains, wcat, wall0, wall1, ceil, resc, fade, mem, packed,
    xg, acc, cs, cr, summed, ms, mg, xw, x1s, xr1, fin,
    load_sem, swap_send, swap_recv, a_send, a_recv, c_send, c_recv, e_send, e_recv, f_send, f_recv,
    w_send, w_recv, l_send, l_recv, far_sem,
):
    t = lax.axis_index("tp")
    d = lax.axis_index("dp")
    z = d // 2
    c = d % 2
    other = 1 - c
    away = (t + NZ - z) % NZ
    past_half = away // 9
    slot_here = (1 - past_half) * (2 * away - (away + 15) // 16) + past_half * (32 - 2 * away)

    barrier = pltpu.get_barrier_semaphore()

    def greet_plane(r, carry):
        to = (t + r) % TP
        pl.semaphore_signal(barrier, inc=1, device_id=(to, z * 2), device_id_type=MESH)
        pl.semaphore_signal(barrier, inc=1, device_id=(to, z * 2 + 1), device_id_type=MESH)
        return carry

    def greet_column(r, carry):
        for to in ((z + r) % NZ, (z + NZ - r) % NZ):
            pl.semaphore_signal(barrier, inc=1, device_id=(t, to * 2 + c), device_id_type=MESH)
        return carry

    lax.fori_loop(1, NEAR + 1, greet_column, 0)
    lax.fori_loop(1, TP, greet_plane, 0)
    pl.semaphore_signal(barrier, inc=1, device_id=(t, z * 2 + other), device_id_type=MESH)

    mine = pl.ds(pl.multiple_of(c * 128, 128), 128)
    weights = (wq, wk, wv, wf, wl, we)
    loads = [
        pltpu.make_async_copy(x_hbm, xin, load_sem.at[0]),
        pltpu.make_async_copy(live_hbm, live_ref, load_sem.at[14]),
    ]
    for p, w in enumerate(weights):
        loads.append(
            pltpu.make_async_copy(w, wcat.at[:, mine, pl.ds(p * 128, 128)], load_sem.at[1 + p])
        )
    loads.append(pltpu.make_async_copy(wo_hbm.at[0], wall0.at[t, :, mine], load_sem.at[7]))
    loads.append(pltpu.make_async_copy(wo_hbm.at[1], wall1.at[t], load_sem.at[13]))
    loads.append(pltpu.make_async_copy(gain_hbm, gains.at[c], load_sem.at[8]))
    loads.append(pltpu.make_async_copy(ceil_hbm, ceil, load_sem.at[9]))
    loads.append(pltpu.make_async_copy(resc_hbm, resc, load_sem.at[10]))
    loads.append(pltpu.make_async_copy(mem_hbm, mem, load_sem.at[11]))
    loads.append(pltpu.make_async_copy(fade_hbm, fade, load_sem.at[12]))
    for copy in loads:
        copy.start()

    lane = lax.broadcasted_iota(jnp.int32, (8, 128), 1)
    low_half = lane < 64
    row_at = lax.broadcasted_iota(jnp.int32, (256, 128), 0)
    lane_at = lax.broadcasted_iota(jnp.int32, (256, 128), 1)
    ones_block = jnp.where((row_at % 128) // 64 == lane_at // 64, 1.0, 0.0).astype(BF16)
    own_row = lax.broadcasted_iota(jnp.int32, (64, 128), 0)
    own_lane = lax.broadcasted_iota(jnp.int32, (64, 128), 1)
    diagonal = (own_lane % 64) == own_row

    def head_sum(x):
        return jnp.dot(split_two(x), ones_block, preferred_element_type=F32)

    loads[0].wait()
    xrows[...] = jnp.zeros((16, 128), F32)
    xrows[0:12, :] = xin[...].astype(F32)
    first = xrows[0:8, :]
    second = xrows[6:14, :]
    xs[0] = first.astype(BF16)
    xs[1] = second.astype(BF16)
    for copy in loads[1:]:
        copy.wait()

    pl.semaphore_wait(barrier, 2 * (TP - 1) + 1 + 2 * NEAR)

    def remote(src, dst, send, recv, to_t, to_z, to_c):
        return pltpu.make_async_remote_copy(
            src_ref=src, dst_ref=dst, send_sem=send, recv_sem=recv,
            device_id=(to_t, to_z * 2 + to_c), device_id_type=MESH,
        )

    def to_sibling(src, i):
        return remote(src, src, swap_send.at[i], swap_recv.at[i], t, z, other)

    def row_copy(to, core):
        return remote(
            xs.at[core], xg.at[c, slot_here], a_send, a_recv, to, z, core
        )

    def row_step(r, carry):
        to = (t + r) % TP
        row_copy(to, 0).start()
        row_copy(to, 1).start()
        return carry

    lax.fori_loop(1, TP, row_step, 0)
    row_copy(t, other).start()
    for to in ((z + NEAR) % NZ, (z + NZ - NEAR) % NZ):
        pl.semaphore_signal(far_sem, inc=1, device_id=(t, to * 2 + c), device_id_type=MESH)
    xg[c, slot_here] = xs[c]

    swaps = [
        to_sibling(gains.at[c], 0),
        to_sibling(wcat.at[0, mine, :], 1),
        to_sibling(wcat.at[1, mine, :], 2),
        to_sibling(wall0.at[:, :, mine], 3),
    ]
    swaps[0].start()
    swaps[1].start()

    def exit_step(r, carry):
        mine_here = wall0.at[t, :, mine]
        remote(mine_here, mine_here, w_send.at[0], w_recv.at[0], (t + r) % TP, z, c).start()
        return carry

    def exit_step_last(r, carry):
        remote(wall1.at[t], wall1.at[t], w_send.at[1], w_recv.at[1], (t + r) % TP, z, c).start()
        return carry

    for b in range(2):
        for s in range(3):
            packed[b, s] = jnp.concatenate([mem[b, s, 0], mem[b, s, 1]], axis=1)

    fade_columns = jnp.transpose(jnp.concatenate([fade[0], fade[1], jnp.zeros((4, 6), F32)], axis=0))

    def all_of(ref, send, recv):
        return remote(ref, ref, send, recv, t, z, other)

    def column(start, first, last):
        if last == 8:
            start((z + 8) % NZ, 15, 15)

        def step(i, carry):
            dist = min(last, 7) - i
            start((z + dist) % NZ, 2 * dist - 1, 2 * dist)
            start((z + NZ - dist) % NZ, 2 * dist, 2 * dist - 1)
            return carry

        lax.fori_loop(0, min(last, 7) - first + 1, step, 0)

    def project(b, rows, lo, hi):
        count = (hi - lo) * 8
        gained = jnp.concatenate(
            [(rows[h] * gains[h, b : b + 1, :].astype(F32)).astype(BF16) for h in range(2)],
            axis=1,
        )
        squares = jnp.sum(rows[0] * rows[0] + rows[1] * rows[1], axis=1, keepdims=True)
        squares = jnp.broadcast_to(squares, (count, 128)).reshape(hi - lo, 8, 128)
        lower = lax.broadcasted_iota(jnp.int32, (hi - lo, 3, 128), 2) < 64
        acc[lo:hi, 36:40, :] = jnp.zeros((hi - lo, 4, 128), F32)
        acc[lo:hi, 36:39, :] = jnp.where(lower, squares[:, 0:3], squares[:, 3:6])
        for p in range(6):
            part = jnp.dot(
                gained, wcat[b, :, p * 128 : (p + 1) * 128], preferred_element_type=F32
            )
            acc[lo:hi, p * 6 : p * 6 + 6, :] = part.reshape(hi - lo, 8, 128)[:, 0:6]
        cs[b, lo:hi] = acc[lo:hi].astype(BF16)

    def send_partials(b, first, last):
        def start(to, here, there):
            remote(cs.at[b, here], cr.at[b, z], c_send.at[b], c_recv.at[b], t, to, c).start()

        column(start, first, last)

    groups = ((0, 7, 1, 3), (7, 13, 4, 6), (13, 16, 7, 8))
    for b in range(2):
        if b == 0:
            swaps[0].wait_recv()
            swaps[1].wait_recv()
            all_of(fin.at[0:31], a_send, a_recv).wait_recv()
            rows = [xg[h].astype(F32).reshape(128, 128) for h in range(2)]
            project(0, rows, 0, 16)
            pl.semaphore_wait(far_sem, 2)
            send_partials(0, 1, 8)
            lax.fori_loop(1, TP, exit_step, 0)
        else:
            swaps[2].wait_recv()
            swaps[3].wait_recv()
            for g, (lo, hi, first, last) in enumerate(groups):
                count = (hi - lo) * 8
                all_of(xw.at[0:15, lo:hi], f_send.at[g], f_recv.at[g]).wait_recv()
                heads = jnp.concatenate(
                    [xw[i, lo:hi].astype(F32).reshape(count, 128).astype(BF16) for i in range(TP)],
                    axis=1,
                )
                mix = jnp.dot(
                    heads, wall0[...].reshape(WIDTH, 256), preferred_element_type=F32
                )
                rows = []
                for h in range(2):
                    before = xg[h, lo:hi].astype(F32).reshape(count, 128)
                    after = (before + mix[:, 128 * h : 128 * h + 128]).astype(BF16).astype(F32)
                    x1s[h, lo:hi] = after.reshape(hi - lo, 8, 128).astype(BF16)
                    rows.append(after)
                project(1, rows, lo, hi)
                send_partials(1, first, last)
            residual = remote(
                x1s.at[other, slot_here], xr1, l_send, l_recv, t, z, other
            )
            residual.start()
            lax.fori_loop(1, TP, exit_step_last, 0)
        own = cs[b, 0]
        cr[b, z] = own

        row8 = lax.broadcasted_iota(jnp.int32, (8, 128), 0)
        live8 = jnp.zeros((8, 128), jnp.int32)
        for s in range(3):
            live8 = jnp.where(row8 // 2 == s, live_ref[s], live8)
        live_rows = (row8 % 2) < live8
        fade8 = jnp.where(low_half[0:6], fade_columns[:, 2 * b : 2 * b + 1], fade_columns[:, 2 * b + 1 : 2 * b + 2])

        all_of(cr.at[b, 0:15], c_send.at[b], c_recv.at[b]).wait_recv()
        summed[0:40, :] = jnp.sum(cr[b].astype(F32), axis=0)
        square_rows = summed[36:39, :]
        low_squares = square_rows[:, 0:1]
        high_squares = square_rows[:, 64:65]
        token_squares = jnp.concatenate([low_squares, high_squares], axis=0)
        row_scale = lax.rsqrt(token_squares / D + NORM_EPS)
        read, key, value, decay_pre, rate_pre, gate_pre = [
            summed[p * 6 : p * 6 + 6, :] * row_scale for p in range(6)
        ]
        decay = jnp.exp(fade8 - ceil[b : b + 1, :] * jax.nn.sigmoid(decay_pre))
        rate = jax.nn.sigmoid(rate_pre)
        gate = jax.nn.sigmoid(gate_pre)
        unit = key * lax.rsqrt(head_sum(key * key) + 1e-06)
        unit_rate = unit * rate
        spread = head_sum(
            jnp.concatenate(
                [jnp.where(diagonal, value[i : i + 1, :], 0.0) for i in range(6)], axis=0
            )
        )
        memory = [packed[b, s] for s in range(3)]
        readouts = [None] * 6
        for j in range(2):
            removed = head_sum(
                jnp.concatenate(
                    [memory[s] * unit[2 * s + j : 2 * s + j + 1, :] for s in range(3)], axis=0
                )
            )
            for s in range(3):
                i = 2 * s + j
                updated = (
                    memory[s] * decay[i : i + 1, :]
                    - removed[64 * s : 64 * s + 64] * unit_rate[i : i + 1, :]
                    + spread[64 * i : 64 * i + 64] * key[i : i + 1, :]
                )
                memory[s] = jnp.where(j < live_ref[s], updated, memory[s])
            read_out = head_sum(
                jnp.concatenate(
                    [memory[s] * read[2 * s + j : 2 * s + j + 1, :] for s in range(3)], axis=0
                )
            )
            for s in range(3):
                readouts[2 * s + j] = jnp.sum(
                    jnp.where(diagonal, read_out[64 * s : 64 * s + 64], 0.0), axis=0, keepdims=True
                )
        readout = jnp.concatenate(readouts, axis=0)
        centered = readout - head_sum(readout) * (1.0 / 64.0)
        variance = head_sum(centered * centered) * (1.0 / 64.0)
        normed = centered * lax.rsqrt(variance + GROUP_EPS) * resc[b : b + 1, :]
        mixed = jnp.where(live_rows[0:6], normed * gate, 0.0)
        ms[b] = jnp.concatenate([mixed, jnp.zeros((2, 128), F32)], axis=0).astype(BF16)

        if b == 0:
            for g in (2, 1, 0):
                lo, hi, first, last = groups[g]

                def start(to, here, there):
                    remote(
                        ms.at[0], mg.at[there], e_send.at[g], e_recv.at[g], t, to, c
                    ).start()

                column(start, first, last)
            mg[0] = ms[0]
            all_of(wall0.at[0:15, :, mine], w_send.at[0], w_recv.at[0]).wait_recv()
            swaps[3].start()
            swaps[2].start()
        else:
            def start_both(to, here, there):
                for core in range(2):
                    remote(
                        ms.at[1], fin.at[c * TP + t], e_send.at[3], e_recv.at[3], z, to, core
                    ).start()

            column(start_both, 1, 8)

            @pl.when(t == z)
            def _():
                remote(
                    ms.at[1], fin.at[c * TP + t], e_send.at[3], e_recv.at[3], z, z, other
                ).start()
                fin[c * TP + t] = ms[1]

            @pl.when(t != z)
            def _():
                for core in range(2):
                    remote(
                        ms.at[1], fin.at[c * TP + t], e_send.at[3], e_recv.at[3], z, z, core
                    ).start()

        for s in range(3):
            states[b, s, 0] = memory[s][:, 0:64]
            states[b, s, 1] = memory[s][:, 64:128]

        if b == 0:
            for g, (lo, hi, first, last) in enumerate(groups):
                arriving = mg.at[max(lo, 1) : hi]
                all_of(arriving, e_send.at[g], e_recv.at[g]).wait_recv()

                def forward(r, carry):
                    remote(
                        mg.at[lo:hi], xw.at[t, lo:hi], f_send.at[g], f_recv.at[g],
                        (t + r) % TP, z, c,
                    ).start()
                    return carry

                lax.fori_loop(1, TP, forward, 0)
                xw[t, lo:hi] = mg[lo:hi]

    all_of(wall1.at[0:15], w_send.at[1], w_recv.at[1]).wait_recv()
    residual.wait_recv()

    @pl.when(t == z)
    def _():
        all_of(fin.at[0:31], e_send.at[3], e_recv.at[3]).wait_recv()

    @pl.when(t != z)
    def _():
        all_of(fin, e_send.at[3], e_recv.at[3]).wait_recv()

    heads = jnp.concatenate(
        [
            jnp.concatenate([fin[i].astype(F32), fin[TP + i].astype(F32)], axis=0).astype(BF16)
            for i in range(TP)
        ],
        axis=1,
    )
    mix = jnp.dot(heads, wall1[...].reshape(WIDTH, 128), preferred_element_type=F32)
    here_rows = x1s[c, slot_here].astype(F32)
    there_rows = xr1[...].astype(F32)
    core = jnp.full((8, 128), c, jnp.int32)
    xrows[0:6, :] = (jnp.where(core == 0, here_rows, there_rows) + mix[0:8])[0:6]
    xrows[6:12, :] = (jnp.where(core == 0, there_rows, here_rows) + mix[8:16])[0:6]
    out_ref[...] = xrows[0:12, :].astype(BF16)

    for copy in swaps:
        copy.wait_send()
    residual.wait_send()
    all_of(fin.at[0:31], a_send, a_recv).wait_send()
    all_of(wall0.at[0:15, :, mine], w_send.at[0], w_recv.at[0]).wait_send()
    all_of(wall1.at[0:15], w_send.at[1], w_recv.at[1]).wait_send()
    for b in range(2):
        all_of(cr.at[b, 0:15], c_send.at[b], c_recv.at[b]).wait_send()
    for g, (lo, hi, first, last) in enumerate(groups):
        all_of(mg.at[max(lo, 1) : hi], e_send.at[g], e_recv.at[g]).wait_send()
        all_of(xw.at[0:15, lo:hi], f_send.at[g], f_recv.at[g]).wait_send()

    @pl.when(t == z)
    def _():
        all_of(fin.at[0:31], e_send.at[3], e_recv.at[3]).wait_send()

    @pl.when(t != z)
    def _():
        all_of(fin, e_send.at[3], e_recv.at[3]).wait_send()


def shards(*arrays):
    arrays = arrays[:13] + (jnp.transpose(arrays[13], (0, 2, 1)),)
    arrays = tuple(pltpu.with_memory_space_constraint(a, pltpu.HBM) for a in arrays)
    hbm = pl.BlockSpec(memory_space=pltpu.HBM)
    in_specs = [hbm] * 14
    dma = pltpu.SemaphoreType.DMA
    return pl.pallas_call(
        kernel,
        out_shape=(
            pltpu.VMEM((12, 128), BF16),
            pltpu.VMEM((2, 3, 2, 64, 64), F32),
        ),
        in_specs=in_specs,
        out_specs=(pl.BlockSpec(memory_space=pltpu.VMEM),) * 2,
        scratch_shapes=[
            pltpu.SMEM((3,), jnp.int32),
            pltpu.VMEM((12, 128), BF16),
            pltpu.VMEM((16, 128), F32),
            pltpu.VMEM((2, 8, 128), BF16),
            pltpu.VMEM((2, 2, 128), BF16),
            pltpu.VMEM((2, 256, 768), BF16),
            pltpu.VMEM((16, 128, 256), BF16),
            pltpu.VMEM((16, 128, 128), BF16),
            pltpu.VMEM((2, 128), F32),
            pltpu.VMEM((2, 128), F32),
            pltpu.VMEM((2, 2, 6), F32),
            pltpu.VMEM((2, 3, 2, 64, 64), F32),
            pltpu.VMEM((2, 3, 64, 128), F32),
            pltpu.VMEM((2, 16, 8, 128), BF16),
            pltpu.VMEM((16, 40, 128), F32),
            pltpu.VMEM((2, 16, 40, 128), BF16),
            pltpu.VMEM((2, 16, 40, 128), BF16),
            pltpu.VMEM((40, 128), F32),
            pltpu.VMEM((2, 8, 128), BF16),
            pltpu.VMEM((16, 8, 128), BF16),
            pltpu.VMEM((16, 16, 8, 128), BF16),
            pltpu.VMEM((2, 16, 8, 128), BF16),
            pltpu.VMEM((8, 128), BF16),
            pltpu.VMEM((32, 8, 128), BF16),
            dma((15,)),
            dma((4,)),
            dma((4,)),
            dma,
            dma,
            dma((2,)),
            dma((2,)),
            dma((4,)),
            dma((4,)),
            dma((3,)),
            dma((3,)),
            dma((2,)),
            dma((2,)),
            dma,
            dma,
            pltpu.SemaphoreType.REGULAR,
        ],
        compiler_params=pltpu.CompilerParams(collective_id=0, has_side_effects=True, vmem_limit_bytes=24 * 1024 * 1024),
    )(*arrays)


def solution(mesh):
    in_specs = (
        P("tp", "dp"),
        P("dp"),
        P(None, "dp"),
        P(None, "dp", "tp"),
        P(None, "dp", "tp"),
        P(None, "dp", "tp"),
        P(None, "dp", "tp"),
        P(None, "dp", "tp"),
        P(None, "dp", "tp"),
        P(None, "tp"),
        P(None, "tp"),
        P(None, "tp", "dp"),
        P(None, "dp", "tp", None, None),
        P(None, "dp", "tp"),
    )
    out_specs = (P("tp", "dp"), P(None, "dp", "tp", None, None))
    return jax.shard_map(shards, mesh=mesh, in_specs=in_specs, out_specs=out_specs, check_vma=False)
```

```python
import jax
import jax.numpy as jnp
from jax import lax
from jax.experimental import pallas as pl
from jax.experimental.pallas import tpu as pltpu
from jax.sharding import PartitionSpec as P

D = 4096
NORM_EPS = 1e-06
GROUP_EPS = 0.00064
TP = 16
NZ = 16
SIDE = 4
AROUND = sorted(
    ((i, j) for i in range(SIDE) for j in range(SIDE) if i + j > 0),
    key=lambda at: -min(at[0], SIDE - at[0]) - min(at[1], SIDE - at[1]),
)
WIDTH = 2048
F32 = jnp.float32
BF16 = jnp.bfloat16
MESH = pl.DeviceIdType.MESH


def split_two(x):
    hi = x.astype(BF16)
    lo = (x - hi.astype(F32)).astype(BF16)
    return jnp.concatenate([hi, lo], axis=1)


def kernel(
    x_hbm, live_hbm, gain_hbm, wq, wk, wv, wf, wl, we, ceil_hbm, resc_hbm, wo_hbm, mem_hbm, fade_hbm,
    out_ref, states,
    live_ref, xin, xrows, xs, gains, wcat, wall0, wall1, ceil, resc, fade, mem, packed,
    xa, xg, acc, cs, cr, summed, ms, mg, xw, x1s, xr1, fin,
    load_sem, swap_send, swap_recv, a_send, a_recv, c_send, c_recv, e_send, e_recv, f_send, f_recv,
    w_send, w_recv, l_send, l_recv, far_sem,
):
    t = lax.axis_index("tp")
    d = lax.axis_index("dp")
    z = d // 2
    c = d % 2
    other = 1 - c
    away = (t + NZ - z) % NZ
    past_half = away // 9
    slot_here = (1 - past_half) * (2 * away - (away + 15) // 16) + past_half * (32 - 2 * away)

    barrier = pltpu.get_barrier_semaphore()

    y = t // SIDE
    x = t % SIDE

    def in_plane(up, right):
        return ((y + up) % SIDE) * SIDE + (x + right) % SIDE

    def greet(to_t, to_z, to_c):
        pl.semaphore_signal(
            barrier, inc=1, device_id=(to_t, to_z * 2 + to_c), device_id_type=MESH
        )

    for r in (2, 1, 3):
        greet(in_plane(0, r), z, 0)
        greet(in_plane(0, r), z, 1)
        greet(in_plane(r, 0), z, c)
    for r in (2, NZ - 2, 1, NZ - 1):
        greet(t, (z + r) % NZ, c)
    pl.semaphore_signal(barrier, inc=1, device_id=(t, z * 2 + other), device_id_type=MESH)

    mine = pl.ds(pl.multiple_of(c * 128, 128), 128)
    weights = (wq, wk, wv, wf, wl, we)
    loads = [
        pltpu.make_async_copy(x_hbm, xin, load_sem.at[0]),
        pltpu.make_async_copy(live_hbm, live_ref, load_sem.at[14]),
    ]
    for p, w in enumerate(weights):
        loads.append(
            pltpu.make_async_copy(w, wcat.at[:, mine, pl.ds(p * 128, 128)], load_sem.at[1 + p])
        )
    loads.append(pltpu.make_async_copy(wo_hbm.at[0], wall0.at[t, :, mine], load_sem.at[7]))
    loads.append(pltpu.make_async_copy(wo_hbm.at[1], wall1.at[t], load_sem.at[13]))
    loads.append(pltpu.make_async_copy(gain_hbm, gains.at[c], load_sem.at[8]))
    loads.append(pltpu.make_async_copy(ceil_hbm, ceil, load_sem.at[9]))
    loads.append(pltpu.make_async_copy(resc_hbm, resc, load_sem.at[10]))
    loads.append(pltpu.make_async_copy(mem_hbm, mem, load_sem.at[11]))
    loads.append(pltpu.make_async_copy(fade_hbm, fade, load_sem.at[12]))
    for copy in loads:
        copy.start()

    lane = lax.broadcasted_iota(jnp.int32, (8, 128), 1)
    low_half = lane < 64
    row_at = lax.broadcasted_iota(jnp.int32, (256, 128), 0)
    lane_at = lax.broadcasted_iota(jnp.int32, (256, 128), 1)
    ones_block = jnp.where((row_at % 128) // 64 == lane_at // 64, 1.0, 0.0).astype(BF16)
    own_row = lax.broadcasted_iota(jnp.int32, (64, 128), 0)
    own_lane = lax.broadcasted_iota(jnp.int32, (64, 128), 1)
    diagonal = (own_lane % 64) == own_row

    def head_sum(x):
        return jnp.dot(split_two(x), ones_block, preferred_element_type=F32)

    loads[0].wait()
    xrows[...] = jnp.zeros((16, 128), F32)
    xrows[0:12, :] = xin[...].astype(F32)
    first = xrows[0:8, :]
    second = xrows[6:14, :]
    xs[0] = first.astype(BF16)
    xs[1] = second.astype(BF16)
    for copy in loads[1:]:
        copy.wait()

    pl.semaphore_wait(barrier, 14)

    def remote(src, dst, send, recv, to_t, to_z, to_c):
        return pltpu.make_async_remote_copy(
            src_ref=src, dst_ref=dst, send_sem=send, recv_sem=recv,
            device_id=(to_t, to_z * 2 + to_c), device_id_type=MESH,
        )

    def to_sibling(src, i):
        return remote(src, src, swap_send.at[i], swap_recv.at[i], t, z, other)

    def row_copy(to, core):
        return remote(xs.at[core], xa.at[c, t], a_send.at[0], a_recv.at[0], to, z, core)

    def tell(sem, r):
        for to in ((z + r) % NZ, (z + NZ - r) % NZ):
            pl.semaphore_signal(sem, inc=1, device_id=(t, to * 2 + c), device_id_type=MESH)

    for r in (2, 1, 3):
        row_copy(in_plane(0, r), 0).start()
        row_copy(in_plane(0, r), 1).start()
    row_copy(t, other).start()
    tell(far_sem.at[0], 2)
    xa[c, t] = xs[c]

    swaps = [
        to_sibling(gains.at[c], 0),
        to_sibling(wcat.at[0, mine, :], 1),
        to_sibling(wcat.at[1, mine, :], 2),
        to_sibling(wall0.at[:, :, mine], 3),
    ]
    swaps[0].start()
    swaps[1].start()

    def exit_step(r, carry):
        mine_here = wall0.at[t, :, mine]
        remote(mine_here, mine_here, w_send.at[0], w_recv.at[0], (t + r) % TP, z, c).start()
        return carry

    def exit_step_last(r, carry):
        remote(wall1.at[t], wall1.at[t], w_send.at[1], w_recv.at[1], (t + r) % TP, z, c).start()
        return carry

    for b in range(2):
        for s in range(3):
            packed[b, s] = jnp.concatenate([mem[b, s, 0], mem[b, s, 1]], axis=1)

    fade_columns = jnp.transpose(jnp.concatenate([fade[0], fade[1], jnp.zeros((4, 6), F32)], axis=0))

    def all_of(ref, send, recv):
        return remote(ref, ref, send, recv, t, z, other)

    def column(start, first, last):
        if last == 8:
            start((z + 8) % NZ, 15, 15)

        def step(i, carry):
            dist = min(last, 7) - i
            start((z + dist) % NZ, 2 * dist - 1, 2 * dist)
            start((z + NZ - dist) % NZ, 2 * dist, 2 * dist - 1)
            return carry

        lax.fori_loop(0, min(last, 7) - first + 1, step, 0)

    def project(b, rows, lo, hi):
        count = (hi - lo) * 8
        gained = jnp.concatenate(
            [(rows[h] * gains[h, b : b + 1, :].astype(F32)).astype(BF16) for h in range(2)],
            axis=1,
        )
        squares = jnp.sum(rows[0] * rows[0] + rows[1] * rows[1], axis=1, keepdims=True)
        squares = jnp.broadcast_to(squares, (count, 128)).reshape(hi - lo, 8, 128)
        lower = lax.broadcasted_iota(jnp.int32, (hi - lo, 3, 128), 2) < 64
        acc[lo:hi, 36:40, :] = jnp.zeros((hi - lo, 4, 128), F32)
        acc[lo:hi, 36:39, :] = jnp.where(lower, squares[:, 0:3], squares[:, 3:6])
        for p in range(6):
            part = jnp.dot(
                gained, wcat[b, :, p * 128 : (p + 1) * 128], preferred_element_type=F32
            )
            acc[lo:hi, p * 6 : p * 6 + 6, :] = part.reshape(hi - lo, 8, 128)[:, 0:6]
        cs[b, lo:hi] = acc[lo:hi].astype(BF16)

    def send_partials(b, first, last):
        def start(to, here, there):
            remote(cs.at[b, here], cr.at[b, z], c_send.at[b], c_recv.at[b], t, to, c).start()

        column(start, first, last)

    groups = ((0, 7, 1, 3), (7, 13, 4, 6), (13, 16, 7, 8))
    for b in range(2):
        if b == 0:
            pl.semaphore_wait(far_sem.at[0], 2)
            tell(far_sem.at[1], 4)
            all_of(fin.at[0:7], a_send.at[0], a_recv.at[0]).wait_recv()
            line = xa.at[:, pl.ds(y * SIDE, SIDE)]
            for r in (2, 1, 3):
                remote(
                    line, line, a_send.at[1], a_recv.at[1], in_plane(r, 0), z, c
                ).start()
            swaps[0].wait_recv()
            swaps[1].wait_recv()
            all_of(fin.at[0:24], a_send.at[1], a_recv.at[1]).wait_recv()
            order = [z] + [
                (z + ((k + 1) // 2 if k % 2 else NZ - k // 2)) % NZ for k in range(1, NZ)
            ]
            rows = []
            for h in range(2):
                tiles = [xa[h, at] for at in order]
                for k in range(NZ):
                    xg[h, k] = tiles[k]
                rows.append(jnp.concatenate([tile.astype(F32) for tile in tiles], axis=0))
            project(0, rows, 0, 16)
            pl.semaphore_wait(far_sem.at[1], 2)
            send_partials(0, 1, 8)
            lax.fori_loop(1, TP, exit_step, 0)
        else:
            swaps[2].wait_recv()
            swaps[3].wait_recv()
            for g, (lo, hi, first, last) in enumerate(groups):
                count = (hi - lo) * 8
                all_of(xw.at[0:15, lo:hi], f_send.at[g], f_recv.at[g]).wait_recv()
                heads = jnp.concatenate(
                    [xw[i, lo:hi].astype(F32).reshape(count, 128).astype(BF16) for i in range(TP)],
                    axis=1,
                )
                mix = jnp.dot(
                    heads, wall0[...].reshape(WIDTH, 256), preferred_element_type=F32
                )
                rows = []
                for h in range(2):
                    before = xg[h, lo:hi].astype(F32).reshape(count, 128)
                    after = (before + mix[:, 128 * h : 128 * h + 128]).astype(BF16).astype(F32)
                    x1s[h, lo:hi] = after.reshape(hi - lo, 8, 128).astype(BF16)
                    rows.append(after)
                project(1, rows, lo, hi)
                send_partials(1, first, last)
            residual = remote(
                x1s.at[other, slot_here], xr1, l_send, l_recv, t, z, other
            )
            residual.start()
            lax.fori_loop(1, TP, exit_step_last, 0)
        own = cs[b, 0]
        cr[b, z] = own

        row8 = lax.broadcasted_iota(jnp.int32, (8, 128), 0)
        live8 = jnp.zeros((8, 128), jnp.int32)
        for s in range(3):
            live8 = jnp.where(row8 // 2 == s, live_ref[s], live8)
        live_rows = (row8 % 2) < live8
        fade8 = jnp.where(low_half[0:6], fade_columns[:, 2 * b : 2 * b + 1], fade_columns[:, 2 * b + 1 : 2 * b + 2])

        all_of(cr.at[b, 0:15], c_send.at[b], c_recv.at[b]).wait_recv()
        summed[0:40, :] = jnp.sum(cr[b].astype(F32), axis=0)
        square_rows = summed[36:39, :]
        low_squares = square_rows[:, 0:1]
        high_squares = square_rows[:, 64:65]
        token_squares = jnp.concatenate([low_squares, high_squares], axis=0)
        row_scale = lax.rsqrt(token_squares / D + NORM_EPS)
        read, key, value, decay_pre, rate_pre, gate_pre = [
            summed[p * 6 : p * 6 + 6, :] * row_scale for p in range(6)
        ]
        decay = jnp.exp(fade8 - ceil[b : b + 1, :] * jax.nn.sigmoid(decay_pre))
        rate = jax.nn.sigmoid(rate_pre)
        gate = jax.nn.sigmoid(gate_pre)
        unit = key * lax.rsqrt(head_sum(key * key) + 1e-06)
        unit_rate = unit * rate
        spread = head_sum(
            jnp.concatenate(
                [jnp.where(diagonal, value[i : i + 1, :], 0.0) for i in range(6)], axis=0
            )
        )
        memory = [packed[b, s] for s in range(3)]
        readouts = [None] * 6
        for j in range(2):
            removed = head_sum(
                jnp.concatenate(
                    [memory[s] * unit[2 * s + j : 2 * s + j + 1, :] for s in range(3)], axis=0
                )
            )
            for s in range(3):
                i = 2 * s + j
                updated = (
                    memory[s] * decay[i : i + 1, :]
                    - removed[64 * s : 64 * s + 64] * unit_rate[i : i + 1, :]
                    + spread[64 * i : 64 * i + 64] * key[i : i + 1, :]
                )
                memory[s] = jnp.where(j < live_ref[s], updated, memory[s])
            read_out = head_sum(
                jnp.concatenate(
                    [memory[s] * read[2 * s + j : 2 * s + j + 1, :] for s in range(3)], axis=0
                )
            )
            for s in range(3):
                readouts[2 * s + j] = jnp.sum(
                    jnp.where(diagonal, read_out[64 * s : 64 * s + 64], 0.0), axis=0, keepdims=True
                )
        readout = jnp.concatenate(readouts, axis=0)
        centered = readout - head_sum(readout) * (1.0 / 64.0)
        variance = head_sum(centered * centered) * (1.0 / 64.0)
        normed = centered * lax.rsqrt(variance + GROUP_EPS) * resc[b : b + 1, :]
        mixed = jnp.where(live_rows[0:6], normed * gate, 0.0)
        ms[b] = jnp.concatenate([mixed, jnp.zeros((2, 128), F32)], axis=0).astype(BF16)

        if b == 0:
            for g in (2, 1, 0):
                lo, hi, first, last = groups[g]

                def start(to, here, there):
                    remote(
                        ms.at[0], mg.at[there], e_send.at[g], e_recv.at[g], t, to, c
                    ).start()

                column(start, first, last)
            mg[0] = ms[0]
            all_of(wall0.at[0:15, :, mine], w_send.at[0], w_recv.at[0]).wait_recv()
            swaps[3].start()
            swaps[2].start()
        else:
            def start_both(to, here, there):
                for core in range(2):
                    remote(
                        ms.at[1], fin.at[c * TP + t], e_send.at[3], e_recv.at[3], z, to, core
                    ).start()

            column(start_both, 1, 8)

            @pl.when(t == z)
            def _():
                remote(
                    ms.at[1], fin.at[c * TP + t], e_send.at[3], e_recv.at[3], z, z, other
                ).start()
                fin[c * TP + t] = ms[1]

            @pl.when(t != z)
            def _():
                for core in range(2):
                    remote(
                        ms.at[1], fin.at[c * TP + t], e_send.at[3], e_recv.at[3], z, z, core
                    ).start()

        for s in range(3):
            states[b, s, 0] = memory[s][:, 0:64]
            states[b, s, 1] = memory[s][:, 64:128]

        if b == 0:
            for g, (lo, hi, first, last) in enumerate(groups):
                arriving = mg.at[max(lo, 1) : hi]
                all_of(arriving, e_send.at[g], e_recv.at[g]).wait_recv()

                for up, right in AROUND:
                    remote(
                        mg.at[lo:hi], xw.at[t, lo:hi], f_send.at[g], f_recv.at[g],
                        in_plane(up, right), z, c,
                    ).start()
                xw[t, lo:hi] = mg[lo:hi]

    all_of(wall1.at[0:15], w_send.at[1], w_recv.at[1]).wait_recv()
    residual.wait_recv()

    @pl.when(t == z)
    def _():
        all_of(fin.at[0:31], e_send.at[3], e_recv.at[3]).wait_recv()

    @pl.when(t != z)
    def _():
        all_of(fin, e_send.at[3], e_recv.at[3]).wait_recv()

    heads = jnp.concatenate(
        [
            jnp.concatenate([fin[i].astype(F32), fin[TP + i].astype(F32)], axis=0).astype(BF16)
            for i in range(TP)
        ],
        axis=1,
    )
    mix = jnp.dot(heads, wall1[...].reshape(WIDTH, 128), preferred_element_type=F32)
    here_rows = x1s[c, slot_here].astype(F32)
    there_rows = xr1[...].astype(F32)
    core = jnp.full((8, 128), c, jnp.int32)
    xrows[0:6, :] = (jnp.where(core == 0, here_rows, there_rows) + mix[0:8])[0:6]
    xrows[6:12, :] = (jnp.where(core == 0, there_rows, here_rows) + mix[8:16])[0:6]
    out_ref[...] = xrows[0:12, :].astype(BF16)

    for copy in swaps:
        copy.wait_send()
    residual.wait_send()
    all_of(fin.at[0:7], a_send.at[0], a_recv.at[0]).wait_send()
    all_of(fin.at[0:24], a_send.at[1], a_recv.at[1]).wait_send()
    all_of(wall0.at[0:15, :, mine], w_send.at[0], w_recv.at[0]).wait_send()
    all_of(wall1.at[0:15], w_send.at[1], w_recv.at[1]).wait_send()
    for b in range(2):
        all_of(cr.at[b, 0:15], c_send.at[b], c_recv.at[b]).wait_send()
    for g, (lo, hi, first, last) in enumerate(groups):
        all_of(mg.at[max(lo, 1) : hi], e_send.at[g], e_recv.at[g]).wait_send()
        all_of(xw.at[0:15, lo:hi], f_send.at[g], f_recv.at[g]).wait_send()

    @pl.when(t == z)
    def _():
        all_of(fin.at[0:31], e_send.at[3], e_recv.at[3]).wait_send()

    @pl.when(t != z)
    def _():
        all_of(fin, e_send.at[3], e_recv.at[3]).wait_send()


def shards(*arrays):
    arrays = arrays[:13] + (jnp.transpose(arrays[13], (0, 2, 1)),)
    arrays = tuple(pltpu.with_memory_space_constraint(a, pltpu.HBM) for a in arrays)
    hbm = pl.BlockSpec(memory_space=pltpu.HBM)
    in_specs = [hbm] * 14
    dma = pltpu.SemaphoreType.DMA
    return pl.pallas_call(
        kernel,
        out_shape=(
            pltpu.VMEM((12, 128), BF16),
            pltpu.VMEM((2, 3, 2, 64, 64), F32),
        ),
        in_specs=in_specs,
        out_specs=(pl.BlockSpec(memory_space=pltpu.VMEM),) * 2,
        scratch_shapes=[
            pltpu.SMEM((3,), jnp.int32),
            pltpu.VMEM((12, 128), BF16),
            pltpu.VMEM((16, 128), F32),
            pltpu.VMEM((2, 8, 128), BF16),
            pltpu.VMEM((2, 2, 128), BF16),
            pltpu.VMEM((2, 256, 768), BF16),
            pltpu.VMEM((16, 128, 256), BF16),
            pltpu.VMEM((16, 128, 128), BF16),
            pltpu.VMEM((2, 128), F32),
            pltpu.VMEM((2, 128), F32),
            pltpu.VMEM((2, 2, 6), F32),
            pltpu.VMEM((2, 3, 2, 64, 64), F32),
            pltpu.VMEM((2, 3, 64, 128), F32),
            pltpu.VMEM((2, 16, 8, 128), BF16),
            pltpu.VMEM((2, 16, 8, 128), BF16),
            pltpu.VMEM((16, 40, 128), F32),
            pltpu.VMEM((2, 16, 40, 128), BF16),
            pltpu.VMEM((2, 16, 40, 128), BF16),
            pltpu.VMEM((40, 128), F32),
            pltpu.VMEM((2, 8, 128), BF16),
            pltpu.VMEM((16, 8, 128), BF16),
            pltpu.VMEM((16, 16, 8, 128), BF16),
            pltpu.VMEM((2, 16, 8, 128), BF16),
            pltpu.VMEM((8, 128), BF16),
            pltpu.VMEM((32, 8, 128), BF16),
            dma((15,)),
            dma((4,)),
            dma((4,)),
            dma((2,)),
            dma((2,)),
            dma((2,)),
            dma((2,)),
            dma((4,)),
            dma((4,)),
            dma((3,)),
            dma((3,)),
            dma((2,)),
            dma((2,)),
            dma,
            dma,
            pltpu.SemaphoreType.REGULAR((2,)),
        ],
        compiler_params=pltpu.CompilerParams(collective_id=0, has_side_effects=True, vmem_limit_bytes=24 * 1024 * 1024),
    )(*arrays)


def solution(mesh):
    in_specs = (
        P("tp", "dp"),
        P("dp"),
        P(None, "dp"),
        P(None, "dp", "tp"),
        P(None, "dp", "tp"),
        P(None, "dp", "tp"),
        P(None, "dp", "tp"),
        P(None, "dp", "tp"),
        P(None, "dp", "tp"),
        P(None, "tp"),
        P(None, "tp"),
        P(None, "tp", "dp"),
        P(None, "dp", "tp", None, None),
        P(None, "dp", "tp"),
    )
    out_specs = (P("tp", "dp"), P(None, "dp", "tp", None, None))
    return jax.shard_map(shards, mesh=mesh, in_specs=in_specs, out_specs=out_specs, check_vma=False)
```

```python
import jax
import jax.numpy as jnp
from jax import lax
from jax.experimental import pallas as pl
from jax.experimental.pallas import tpu as pltpu
from jax.sharding import PartitionSpec as P

D = 4096
NORM_EPS = 1e-06
GROUP_EPS = 0.00064
TP = 16
NZ = 16
SIDE = 4
AROUND = sorted(
    ((i, j) for i in range(SIDE) for j in range(SIDE) if i + j > 0),
    key=lambda at: -min(at[0], SIDE - at[0]) - min(at[1], SIDE - at[1]),
)
WIDTH = 2048
F32 = jnp.float32
BF16 = jnp.bfloat16
MESH = pl.DeviceIdType.MESH


def split_two(x):
    hi = x.astype(BF16)
    lo = (x - hi.astype(F32)).astype(BF16)
    return jnp.concatenate([hi, lo], axis=1)


def kernel(
    x_hbm, live_hbm, gain_hbm, wq, wk, wv, wf, wl, we, ceil_hbm, resc_hbm, wo_hbm, mem_hbm, fade_hbm,
    out_ref, states,
    live_ref, xin, xrows, xs, gains, wcat, wall0, wall1, ceil, resc, fade, mem, packed,
    xa, xg, acc, cs, cr, summed, ms, mg, xw, x1s, xr1, fin,
    load_sem, swap_send, swap_recv, a_send, a_recv, c_send, c_recv, e_send, e_recv, f_send, f_recv,
    w_send, w_recv, l_send, l_recv, far_sem,
):
    t = lax.axis_index("tp")
    d = lax.axis_index("dp")
    z = d // 2
    c = d % 2
    other = 1 - c
    away = (t + NZ - z) % NZ
    past_half = away // 9
    slot_here = (1 - past_half) * (2 * away - (away + 15) // 16) + past_half * (32 - 2 * away)

    barrier = pltpu.get_barrier_semaphore()

    load_rows = pltpu.make_async_copy(x_hbm, xin, load_sem.at[0])
    load_rows.start()
    y = t // SIDE
    x = t % SIDE

    def in_plane(up, right):
        return ((y + up) % SIDE) * SIDE + (x + right) % SIDE

    def greet(to_t, to_z, to_c):
        pl.semaphore_signal(
            barrier, inc=1, device_id=(to_t, to_z * 2 + to_c), device_id_type=MESH
        )

    for r in (2, 1, 3):
        greet(in_plane(0, r), z, 0)
        greet(in_plane(0, r), z, 1)
        greet(in_plane(r, 0), z, c)
    for r in (2, NZ - 2, 1, NZ - 1):
        greet(t, (z + r) % NZ, c)
    pl.semaphore_signal(barrier, inc=1, device_id=(t, z * 2 + other), device_id_type=MESH)

    mine = pl.ds(pl.multiple_of(c * 128, 128), 128)
    weights = (wq, wk, wv, wf, wl, we)
    loads = [pltpu.make_async_copy(live_hbm, live_ref, load_sem.at[14])]
    for p, w in enumerate(weights):
        loads.append(
            pltpu.make_async_copy(w, wcat.at[:, mine, pl.ds(p * 128, 128)], load_sem.at[1 + p])
        )
    loads.append(pltpu.make_async_copy(wo_hbm.at[0], wall0.at[t, :, mine], load_sem.at[7]))
    loads.append(pltpu.make_async_copy(wo_hbm.at[1], wall1.at[t], load_sem.at[13]))
    loads.append(pltpu.make_async_copy(gain_hbm, gains.at[c], load_sem.at[8]))
    loads.append(pltpu.make_async_copy(ceil_hbm, ceil, load_sem.at[9]))
    loads.append(pltpu.make_async_copy(resc_hbm, resc, load_sem.at[10]))
    loads.append(pltpu.make_async_copy(mem_hbm, mem, load_sem.at[11]))
    loads.append(pltpu.make_async_copy(fade_hbm, fade, load_sem.at[12]))
    for copy in loads:
        copy.start()

    lane = lax.broadcasted_iota(jnp.int32, (8, 128), 1)
    low_half = lane < 64
    row_at = lax.broadcasted_iota(jnp.int32, (256, 128), 0)
    lane_at = lax.broadcasted_iota(jnp.int32, (256, 128), 1)
    ones_block = jnp.where((row_at % 128) // 64 == lane_at // 64, 1.0, 0.0).astype(BF16)
    own_row = lax.broadcasted_iota(jnp.int32, (64, 128), 0)
    own_lane = lax.broadcasted_iota(jnp.int32, (64, 128), 1)
    diagonal = (own_lane % 64) == own_row

    def head_sum(x):
        return jnp.dot(split_two(x), ones_block, preferred_element_type=F32)

    load_rows.wait()
    xrows[...] = jnp.zeros((16, 128), F32)
    xrows[0:12, :] = xin[...].astype(F32)
    first = xrows[0:8, :]
    second = xrows[6:14, :]
    xs[0] = first.astype(BF16)
    xs[1] = second.astype(BF16)
    pl.semaphore_wait(barrier, 14)

    def remote(src, dst, send, recv, to_t, to_z, to_c):
        return pltpu.make_async_remote_copy(
            src_ref=src, dst_ref=dst, send_sem=send, recv_sem=recv,
            device_id=(to_t, to_z * 2 + to_c), device_id_type=MESH,
        )

    def to_sibling(src, i):
        return remote(src, src, swap_send.at[i], swap_recv.at[i], t, z, other)

    def row_copy(to, core):
        return remote(xs.at[core], xa.at[c, t], a_send.at[0], a_recv.at[0], to, z, core)

    def tell(sem, r):
        for to in ((z + r) % NZ, (z + NZ - r) % NZ):
            pl.semaphore_signal(sem, inc=1, device_id=(t, to * 2 + c), device_id_type=MESH)

    for r in (2, 1, 3):
        row_copy(in_plane(0, r), 0).start()
        row_copy(in_plane(0, r), 1).start()
    row_copy(t, other).start()
    tell(far_sem.at[0], 2)
    xa[c, t] = xs[c]

    swaps = [
        to_sibling(gains.at[c], 0),
        to_sibling(wcat.at[0, mine, :], 1),
        to_sibling(wcat.at[1, mine, :], 2),
        to_sibling(wall0.at[:, :, mine], 3),
    ]
    for copy in loads:
        copy.wait()
    swaps[0].start()
    swaps[1].start()

    def exit_step(r, carry):
        mine_here = wall0.at[t, :, mine]
        remote(mine_here, mine_here, w_send.at[0], w_recv.at[0], (t + r) % TP, z, c).start()
        return carry

    def exit_step_last(r, carry):
        remote(wall1.at[t], wall1.at[t], w_send.at[1], w_recv.at[1], (t + r) % TP, z, c).start()
        return carry

    for b in range(2):
        for s in range(3):
            packed[b, s] = jnp.concatenate([mem[b, s, 0], mem[b, s, 1]], axis=1)

    fade_columns = jnp.transpose(jnp.concatenate([fade[0], fade[1], jnp.zeros((4, 6), F32)], axis=0))

    def all_of(ref, send, recv):
        return remote(ref, ref, send, recv, t, z, other)

    def column(start, first, last):
        if last == 8:
            start((z + 8) % NZ, 15, 15)

        def step(i, carry):
            dist = min(last, 7) - i
            start((z + dist) % NZ, 2 * dist - 1, 2 * dist)
            start((z + NZ - dist) % NZ, 2 * dist, 2 * dist - 1)
            return carry

        lax.fori_loop(0, min(last, 7) - first + 1, step, 0)

    def project(b, rows, lo, hi):
        count = (hi - lo) * 8
        gained = jnp.concatenate(
            [(rows[h] * gains[h, b : b + 1, :].astype(F32)).astype(BF16) for h in range(2)],
            axis=1,
        )
        squares = jnp.sum(rows[0] * rows[0] + rows[1] * rows[1], axis=1, keepdims=True)
        squares = jnp.broadcast_to(squares, (count, 128)).reshape(hi - lo, 8, 128)
        lower = lax.broadcasted_iota(jnp.int32, (hi - lo, 3, 128), 2) < 64
        acc[lo:hi, 36:40, :] = jnp.zeros((hi - lo, 4, 128), F32)
        acc[lo:hi, 36:39, :] = jnp.where(lower, squares[:, 0:3], squares[:, 3:6])
        for p in range(6):
            part = jnp.dot(
                gained, wcat[b, :, p * 128 : (p + 1) * 128], preferred_element_type=F32
            )
            acc[lo:hi, p * 6 : p * 6 + 6, :] = part.reshape(hi - lo, 8, 128)[:, 0:6]
        cs[b, lo:hi] = acc[lo:hi].astype(BF16)

    def send_partials(b, first, last):
        def start(to, here, there):
            remote(cs.at[b, here], cr.at[b, z], c_send.at[b], c_recv.at[b], t, to, c).start()

        column(start, first, last)

    groups = ((0, 7, 1, 3), (7, 13, 4, 6), (13, 16, 7, 8))
    for b in range(2):
        if b == 0:
            pl.semaphore_wait(far_sem.at[0], 2)
            tell(far_sem.at[1], 4)
            all_of(fin.at[0:7], a_send.at[0], a_recv.at[0]).wait_recv()
            line = xa.at[:, pl.ds(y * SIDE, SIDE)]
            for r in (2, 1, 3):
                remote(
                    line, line, a_send.at[1], a_recv.at[1], in_plane(r, 0), z, c
                ).start()
            swaps[0].wait_recv()
            swaps[1].wait_recv()
            all_of(fin.at[0:24], a_send.at[1], a_recv.at[1]).wait_recv()
            order = [z] + [
                (z + ((k + 1) // 2 if k % 2 else NZ - k // 2)) % NZ for k in range(1, NZ)
            ]
            rows = []
            for h in range(2):
                tiles = [xa[h, at] for at in order]
                for k in range(NZ):
                    xg[h, k] = tiles[k]
                rows.append(jnp.concatenate([tile.astype(F32) for tile in tiles], axis=0))
            project(0, rows, 0, 16)
            pl.semaphore_wait(far_sem.at[1], 2)
            send_partials(0, 1, 8)
            lax.fori_loop(1, TP, exit_step, 0)
        else:
            swaps[2].wait_recv()
            swaps[3].wait_recv()
            for g, (lo, hi, first, last) in enumerate(groups):
                count = (hi - lo) * 8
                all_of(xw.at[0:15, lo:hi], f_send.at[g], f_recv.at[g]).wait_recv()
                heads = jnp.concatenate(
                    [xw[i, lo:hi].astype(F32).reshape(count, 128).astype(BF16) for i in range(TP)],
                    axis=1,
                )
                mix = jnp.dot(
                    heads, wall0[...].reshape(WIDTH, 256), preferred_element_type=F32
                )
                rows = []
                for h in range(2):
                    before = xg[h, lo:hi].astype(F32).reshape(count, 128)
                    after = (before + mix[:, 128 * h : 128 * h + 128]).astype(BF16).astype(F32)
                    x1s[h, lo:hi] = after.reshape(hi - lo, 8, 128).astype(BF16)
                    rows.append(after)
                project(1, rows, lo, hi)
                send_partials(1, first, last)
            residual = remote(
                x1s.at[other, slot_here], xr1, l_send, l_recv, t, z, other
            )
            residual.start()
            lax.fori_loop(1, TP, exit_step_last, 0)
        own = cs[b, 0]
        cr[b, z] = own

        row8 = lax.broadcasted_iota(jnp.int32, (8, 128), 0)
        live8 = jnp.zeros((8, 128), jnp.int32)
        for s in range(3):
            live8 = jnp.where(row8 // 2 == s, live_ref[s], live8)
        live_rows = (row8 % 2) < live8
        fade8 = jnp.where(low_half[0:6], fade_columns[:, 2 * b : 2 * b + 1], fade_columns[:, 2 * b + 1 : 2 * b + 2])

        all_of(cr.at[b, 0:15], c_send.at[b], c_recv.at[b]).wait_recv()
        summed[0:40, :] = jnp.sum(cr[b].astype(F32), axis=0)
        square_rows = summed[36:39, :]
        low_squares = square_rows[:, 0:1]
        high_squares = square_rows[:, 64:65]
        token_squares = jnp.concatenate([low_squares, high_squares], axis=0)
        row_scale = lax.rsqrt(token_squares / D + NORM_EPS)
        read, key, value, decay_pre, rate_pre, gate_pre = [
            summed[p * 6 : p * 6 + 6, :] * row_scale for p in range(6)
        ]
        decay = jnp.exp(fade8 - ceil[b : b + 1, :] * jax.nn.sigmoid(decay_pre))
        rate = jax.nn.sigmoid(rate_pre)
        gate = jax.nn.sigmoid(gate_pre)
        removal = key * rate / (head_sum(key * key) + 1e-06)
        spread = head_sum(
            jnp.concatenate(
                [jnp.where(diagonal, value[i : i + 1, :], 0.0) for i in range(6)], axis=0
            )
        )
        memory = [packed[b, s] for s in range(3)]
        readouts = [None] * 6
        spreads = [None] * 6
        for j in range(2):
            removed = head_sum(
                jnp.concatenate(
                    [memory[s] * key[2 * s + j : 2 * s + j + 1, :] for s in range(3)], axis=0
                )
            )
            for s in range(3):
                i = 2 * s + j
                updated = (
                    memory[s] * decay[i : i + 1, :]
                    - removed[64 * s : 64 * s + 64] * removal[i : i + 1, :]
                    + spread[64 * i : 64 * i + 64] * key[i : i + 1, :]
                )
                memory[s] = jnp.where(j < live_ref[s], updated, memory[s])
            read_out = head_sum(
                jnp.concatenate(
                    [memory[s] * read[2 * s + j : 2 * s + j + 1, :] for s in range(3)], axis=0
                )
            )
            for s in range(3):
                here = read_out[64 * s : 64 * s + 64]
                here = here - jnp.sum(here, axis=0, keepdims=True) * (1.0 / 64.0)
                spreads[2 * s + j] = jnp.sum(here * here, axis=0, keepdims=True)
                readouts[2 * s + j] = jnp.sum(
                    jnp.where(diagonal, here, 0.0), axis=0, keepdims=True
                )
        variance = jnp.concatenate(spreads, axis=0) * (1.0 / 64.0)
        centered = jnp.concatenate(readouts, axis=0)
        normed = centered * lax.rsqrt(variance + GROUP_EPS) * resc[b : b + 1, :]
        mixed = jnp.where(live_rows[0:6], normed * gate, 0.0)
        ms[b] = jnp.concatenate([mixed, jnp.zeros((2, 128), F32)], axis=0).astype(BF16)

        if b == 0:
            for g in (2, 1, 0):
                lo, hi, first, last = groups[g]

                def start(to, here, there):
                    remote(
                        ms.at[0], mg.at[there], e_send.at[g], e_recv.at[g], t, to, c
                    ).start()

                column(start, first, last)
            mg[0] = ms[0]
            all_of(wall0.at[0:15, :, mine], w_send.at[0], w_recv.at[0]).wait_recv()
            swaps[3].start()
            swaps[2].start()
        else:
            def start_both(to, here, there):
                for core in range(2):
                    remote(
                        ms.at[1], fin.at[c * TP + t], e_send.at[3], e_recv.at[3], z, to, core
                    ).start()

            column(start_both, 1, 8)

            @pl.when(t == z)
            def _():
                remote(
                    ms.at[1], fin.at[c * TP + t], e_send.at[3], e_recv.at[3], z, z, other
                ).start()
                fin[c * TP + t] = ms[1]

            @pl.when(t != z)
            def _():
                for core in range(2):
                    remote(
                        ms.at[1], fin.at[c * TP + t], e_send.at[3], e_recv.at[3], z, z, core
                    ).start()

        for s in range(3):
            states[b, s, 0] = memory[s][:, 0:64]
            states[b, s, 1] = memory[s][:, 64:128]

        if b == 0:
            for g, (lo, hi, first, last) in enumerate(groups):
                arriving = mg.at[max(lo, 1) : hi]
                all_of(arriving, e_send.at[g], e_recv.at[g]).wait_recv()

                for up, right in AROUND:
                    remote(
                        mg.at[lo:hi], xw.at[t, lo:hi], f_send.at[g], f_recv.at[g],
                        in_plane(up, right), z, c,
                    ).start()
                xw[t, lo:hi] = mg[lo:hi]

    all_of(wall1.at[0:15], w_send.at[1], w_recv.at[1]).wait_recv()
    residual.wait_recv()

    @pl.when(t == z)
    def _():
        all_of(fin.at[0:31], e_send.at[3], e_recv.at[3]).wait_recv()

    @pl.when(t != z)
    def _():
        all_of(fin, e_send.at[3], e_recv.at[3]).wait_recv()

    heads = jnp.concatenate(
        [
            jnp.concatenate([fin[i].astype(F32), fin[TP + i].astype(F32)], axis=0).astype(BF16)
            for i in range(TP)
        ],
        axis=1,
    )
    mix = jnp.dot(heads, wall1[...].reshape(WIDTH, 128), preferred_element_type=F32)
    here_rows = x1s[c, slot_here].astype(F32)
    there_rows = xr1[...].astype(F32)
    core = jnp.full((8, 128), c, jnp.int32)
    xrows[0:6, :] = (jnp.where(core == 0, here_rows, there_rows) + mix[0:8])[0:6]
    xrows[6:12, :] = (jnp.where(core == 0, there_rows, here_rows) + mix[8:16])[0:6]
    out_ref[...] = xrows[0:12, :].astype(BF16)

    for copy in swaps:
        copy.wait_send()
    residual.wait_send()
    all_of(fin.at[0:7], a_send.at[0], a_recv.at[0]).wait_send()
    all_of(fin.at[0:24], a_send.at[1], a_recv.at[1]).wait_send()
    all_of(wall0.at[0:15, :, mine], w_send.at[0], w_recv.at[0]).wait_send()
    all_of(wall1.at[0:15], w_send.at[1], w_recv.at[1]).wait_send()
    for b in range(2):
        all_of(cr.at[b, 0:15], c_send.at[b], c_recv.at[b]).wait_send()
    for g, (lo, hi, first, last) in enumerate(groups):
        all_of(mg.at[max(lo, 1) : hi], e_send.at[g], e_recv.at[g]).wait_send()
        all_of(xw.at[0:15, lo:hi], f_send.at[g], f_recv.at[g]).wait_send()

    @pl.when(t == z)
    def _():
        all_of(fin.at[0:31], e_send.at[3], e_recv.at[3]).wait_send()

    @pl.when(t != z)
    def _():
        all_of(fin, e_send.at[3], e_recv.at[3]).wait_send()


def shards(*arrays):
    arrays = arrays[:13] + (jnp.transpose(arrays[13], (0, 2, 1)),)
    arrays = tuple(pltpu.with_memory_space_constraint(a, pltpu.HBM) for a in arrays)
    hbm = pl.BlockSpec(memory_space=pltpu.HBM)
    in_specs = [hbm] * 14
    dma = pltpu.SemaphoreType.DMA
    return pl.pallas_call(
        kernel,
        out_shape=(
            pltpu.VMEM((12, 128), BF16),
            pltpu.VMEM((2, 3, 2, 64, 64), F32),
        ),
        in_specs=in_specs,
        out_specs=(pl.BlockSpec(memory_space=pltpu.VMEM),) * 2,
        scratch_shapes=[
            pltpu.SMEM((3,), jnp.int32),
            pltpu.VMEM((12, 128), BF16),
            pltpu.VMEM((16, 128), F32),
            pltpu.VMEM((2, 8, 128), BF16),
            pltpu.VMEM((2, 2, 128), BF16),
            pltpu.VMEM((2, 256, 768), BF16),
            pltpu.VMEM((16, 128, 256), BF16),
            pltpu.VMEM((16, 128, 128), BF16),
            pltpu.VMEM((2, 128), F32),
            pltpu.VMEM((2, 128), F32),
            pltpu.VMEM((2, 2, 6), F32),
            pltpu.VMEM((2, 3, 2, 64, 64), F32),
            pltpu.VMEM((2, 3, 64, 128), F32),
            pltpu.VMEM((2, 16, 8, 128), BF16),
            pltpu.VMEM((2, 16, 8, 128), BF16),
            pltpu.VMEM((16, 40, 128), F32),
            pltpu.VMEM((2, 16, 40, 128), BF16),
            pltpu.VMEM((2, 16, 40, 128), BF16),
            pltpu.VMEM((40, 128), F32),
            pltpu.VMEM((2, 8, 128), BF16),
            pltpu.VMEM((16, 8, 128), BF16),
            pltpu.VMEM((16, 16, 8, 128), BF16),
            pltpu.VMEM((2, 16, 8, 128), BF16),
            pltpu.VMEM((8, 128), BF16),
            pltpu.VMEM((32, 8, 128), BF16),
            dma((15,)),
            dma((4,)),
            dma((4,)),
            dma((2,)),
            dma((2,)),
            dma((2,)),
            dma((2,)),
            dma((4,)),
            dma((4,)),
            dma((3,)),
            dma((3,)),
            dma((2,)),
            dma((2,)),
            dma,
            dma,
            pltpu.SemaphoreType.REGULAR((2,)),
        ],
        compiler_params=pltpu.CompilerParams(collective_id=0, has_side_effects=True, vmem_limit_bytes=24 * 1024 * 1024),
    )(*arrays)


def solution(mesh):
    in_specs = (
        P("tp", "dp"),
        P("dp"),
        P(None, "dp"),
        P(None, "dp", "tp"),
        P(None, "dp", "tp"),
        P(None, "dp", "tp"),
        P(None, "dp", "tp"),
        P(None, "dp", "tp"),
        P(None, "dp", "tp"),
        P(None, "tp"),
        P(None, "tp"),
        P(None, "tp", "dp"),
        P(None, "dp", "tp", None, None),
        P(None, "dp", "tp"),
    )
    out_specs = (P("tp", "dp"), P(None, "dp", "tp", None, None))
    return jax.shard_map(shards, mesh=mesh, in_specs=in_specs, out_specs=out_specs, check_vma=False)
```

```python
import jax
import jax.numpy as jnp
from jax import lax
from jax.experimental import pallas as pl
from jax.experimental.pallas import tpu as pltpu
from jax.sharding import PartitionSpec as P

D = 4096
NORM_EPS = 1e-06
GROUP_EPS = 0.00064
TP = 16
NZ = 16
SIDE = 4
AROUND = sorted(
    ((i, j) for i in range(SIDE) for j in range(SIDE) if i + j > 0),
    key=lambda at: -min(at[0], SIDE - at[0]) - min(at[1], SIDE - at[1]),
)
WIDTH = 2048
F32 = jnp.float32
BF16 = jnp.bfloat16
MESH = pl.DeviceIdType.MESH


def split_two(x):
    hi = x.astype(BF16)
    lo = (x - hi.astype(F32)).astype(BF16)
    return jnp.concatenate([hi, lo], axis=1)


def kernel(
    x_hbm, live_hbm, gain_hbm, wq, wk, wv, wf, wl, we, ceil_hbm, resc_hbm, wo_hbm, mem_hbm, fade_hbm,
    out_ref, states,
    live_ref, xin, xrows, xs, gains, wcat, wall0, wall1, ceil, resc, fade, mem, packed,
    xa, xb, xg, acc, cs, cr, summed, ms, mg, xw, x1s, xr1, fin,
    load_sem, swap_send, swap_recv, a_send, a_recv, c_send, c_recv, e_send, e_recv, f_send, f_recv,
    w_send, w_recv, l_send, l_recv, far_sem,
):
    t = lax.axis_index("tp")
    d = lax.axis_index("dp")
    z = d // 2
    c = d % 2
    other = 1 - c
    away = (t + NZ - z) % NZ
    past_half = away // 9
    slot_here = (1 - past_half) * (2 * away - (away + 15) // 16) + past_half * (32 - 2 * away)

    barrier = pltpu.get_barrier_semaphore()

    load_rows = pltpu.make_async_copy(x_hbm, xin, load_sem.at[0])
    load_rows.start()
    y = t // SIDE
    x = t % SIDE

    def in_plane(up, right):
        return ((y + up) % SIDE) * SIDE + (x + right) % SIDE

    def greet(to_t, to_z, to_c):
        pl.semaphore_signal(
            barrier, inc=1, device_id=(to_t, to_z * 2 + to_c), device_id_type=MESH
        )

    for r in (2, 1, 3):
        greet(in_plane(0, r), z, 0)
        greet(in_plane(0, r), z, 1)
        greet(in_plane(r, 0), z, other)
    for r in (2, NZ - 2, 1, NZ - 1):
        greet(t, (z + r) % NZ, 0)
        greet(t, (z + r) % NZ, 1)
    pl.semaphore_signal(barrier, inc=1, device_id=(t, z * 2 + other), device_id_type=MESH)

    mine = pl.ds(pl.multiple_of(c * 128, 128), 128)
    weights = (wq, wk, wv, wf, wl, we)
    loads = [pltpu.make_async_copy(live_hbm, live_ref, load_sem.at[14])]
    for p, w in enumerate(weights):
        loads.append(
            pltpu.make_async_copy(w, wcat.at[:, mine, pl.ds(p * 128, 128)], load_sem.at[1 + p])
        )
    loads.append(pltpu.make_async_copy(wo_hbm.at[0], wall0.at[t, :, mine], load_sem.at[7]))
    loads.append(pltpu.make_async_copy(wo_hbm.at[1], wall1.at[t], load_sem.at[13]))
    loads.append(pltpu.make_async_copy(gain_hbm, gains.at[c], load_sem.at[8]))
    loads.append(pltpu.make_async_copy(ceil_hbm, ceil, load_sem.at[9]))
    loads.append(pltpu.make_async_copy(resc_hbm, resc, load_sem.at[10]))
    loads.append(pltpu.make_async_copy(mem_hbm, mem, load_sem.at[11]))
    loads.append(pltpu.make_async_copy(fade_hbm, fade, load_sem.at[12]))
    for copy in loads:
        copy.start()

    lane = lax.broadcasted_iota(jnp.int32, (8, 128), 1)
    low_half = lane < 64
    row_at = lax.broadcasted_iota(jnp.int32, (256, 128), 0)
    lane_at = lax.broadcasted_iota(jnp.int32, (256, 128), 1)
    ones_block = jnp.where((row_at % 128) // 64 == lane_at // 64, 1.0, 0.0).astype(BF16)
    own_row = lax.broadcasted_iota(jnp.int32, (64, 128), 0)
    own_lane = lax.broadcasted_iota(jnp.int32, (64, 128), 1)
    diagonal = (own_lane % 64) == own_row

    def head_sum(x):
        return jnp.dot(split_two(x), ones_block, preferred_element_type=F32)

    load_rows.wait()
    xrows[...] = jnp.zeros((16, 128), F32)
    xrows[0:12, :] = xin[...].astype(F32)
    first = xrows[0:8, :]
    second = xrows[6:14, :]
    xs[0] = first.astype(BF16)
    xs[1] = second.astype(BF16)
    pl.semaphore_wait(barrier, 18)

    def remote(src, dst, send, recv, to_t, to_z, to_c):
        return pltpu.make_async_remote_copy(
            src_ref=src, dst_ref=dst, send_sem=send, recv_sem=recv,
            device_id=(to_t, to_z * 2 + to_c), device_id_type=MESH,
        )

    def to_sibling(src, i):
        return remote(src, src, swap_send.at[i], swap_recv.at[i], t, z, other)

    def row_copy(to, core):
        return remote(xs.at[core], xa.at[c, t], a_send.at[0], a_recv.at[0], to, z, core)

    def tell(sem, r):
        for to in ((z + r) % NZ, (z + NZ - r) % NZ):
            pl.semaphore_signal(sem, inc=1, device_id=(t, to * 2 + c), device_id_type=MESH)

    for r in (2, 1, 3):
        row_copy(in_plane(0, r), 0).start()
        row_copy(in_plane(0, r), 1).start()
    row_copy(t, other).start()
    tell(far_sem.at[0], 2)
    xa[c, t] = xs[c]

    swaps = [
        to_sibling(gains.at[c], 0),
        to_sibling(wcat.at[0, mine, :], 1),
        to_sibling(wcat.at[1, mine, :], 2),
        to_sibling(wall0.at[:, :, mine], 3),
    ]
    for copy in loads:
        copy.wait()
    swaps[0].start()
    swaps[1].start()

    def exit_step(r, carry):
        mine_here = wall0.at[t, :, mine]
        remote(mine_here, mine_here, w_send.at[0], w_recv.at[0], (t + r) % TP, z, c).start()
        return carry

    def exit_step_last(r, carry):
        remote(wall1.at[t], wall1.at[t], w_send.at[1], w_recv.at[1], (t + r) % TP, z, c).start()
        return carry

    for b in range(2):
        for s in range(3):
            packed[b, s] = jnp.concatenate([mem[b, s, 0], mem[b, s, 1]], axis=1)

    fade_columns = jnp.transpose(jnp.concatenate([fade[0], fade[1], jnp.zeros((4, 6), F32)], axis=0))

    def all_of(ref, send, recv):
        return remote(ref, ref, send, recv, t, z, other)

    def column(start, first, last, whole=True):
        if last == 8:
            start((z + 8) % NZ, 15, 15)

        def step(i, carry):
            dist = min(last, 7) - i
            start((z + dist) % NZ, 2 * dist - 1, 2 * dist)
            start((z + NZ - dist) % NZ, 2 * dist, 2 * dist - 1)
            return carry

        lax.fori_loop(0, min(last, 7) - first + 1, step, 0)
        if first == 1 and whole:
            start(z, 0, 0)

    def project(b, rows, lo, hi):
        count = (hi - lo) * 8
        gained = jnp.concatenate(
            [(rows[h] * gains[h, b : b + 1, :].astype(F32)).astype(BF16) for h in range(2)],
            axis=1,
        )
        squares = jnp.sum(rows[0] * rows[0] + rows[1] * rows[1], axis=1, keepdims=True)
        squares = jnp.broadcast_to(squares, (count, 128)).reshape(hi - lo, 8, 128)
        lower = lax.broadcasted_iota(jnp.int32, (hi - lo, 3, 128), 2) < 64
        acc[lo:hi, 36:40, :] = jnp.zeros((hi - lo, 4, 128), F32)
        acc[lo:hi, 36:39, :] = jnp.where(lower, squares[:, 0:3], squares[:, 3:6])
        for p in range(6):
            part = jnp.dot(
                gained, wcat[b, :, p * 128 : (p + 1) * 128], preferred_element_type=F32
            )
            acc[lo:hi, p * 6 : p * 6 + 6, :] = part.reshape(hi - lo, 8, 128)[:, 0:6]
        cs[b, lo:hi] = acc[lo:hi].astype(BF16)

    def send_partials(b, first, last):
        def start(to, here, there):
            remote(
                cs.at[b, here], cr.at[b, z], c_send.at[b], c_recv.at[b], t, to, other
            ).start()

        column(start, first, last)

    groups = ((0, 7, 1, 3), (7, 13, 4, 6), (13, 16, 7, 8))
    for b in range(2):
        if b == 0:
            pl.semaphore_wait(far_sem.at[0], 2)
            tell(far_sem.at[1], 4)
            all_of(fin.at[0:7], a_send.at[0], a_recv.at[0]).wait_recv()
            line = xa.at[:, pl.ds(y * SIDE, SIDE)]
            there = xb.at[:, pl.ds(y * SIDE, SIDE)]
            for r in (2, 1, 3, 0):
                remote(
                    line, there, a_send.at[1], a_recv.at[1], in_plane(r, 0), z, other
                ).start()
            swaps[0].wait_recv()
            swaps[1].wait_recv()
            all_of(fin, a_send.at[1], a_recv.at[1]).wait_recv()
            order = [z] + [
                (z + ((k + 1) // 2 if k % 2 else NZ - k // 2)) % NZ for k in range(1, NZ)
            ]
            rows = []
            for h in range(2):
                tiles = [xb[h, at] for at in order]
                for k in range(NZ):
                    xg[h, k] = tiles[k]
                rows.append(jnp.concatenate([tile.astype(F32) for tile in tiles], axis=0))
            project(0, rows, 0, 16)
            pl.semaphore_wait(far_sem.at[1], 2)
            send_partials(0, 1, 8)
            lax.fori_loop(1, TP, exit_step, 0)
        else:
            swaps[2].wait_recv()
            swaps[3].wait_recv()
            for g, (lo, hi, first, last) in enumerate(groups):
                count = (hi - lo) * 8
                all_of(xw.at[0:15, lo:hi], f_send.at[g], f_recv.at[g]).wait_recv()
                heads = jnp.concatenate(
                    [xw[i, lo:hi].astype(F32).reshape(count, 128).astype(BF16) for i in range(TP)],
                    axis=1,
                )
                mix = jnp.dot(
                    heads, wall0[...].reshape(WIDTH, 256), preferred_element_type=F32
                )
                rows = []
                for h in range(2):
                    before = xg[h, lo:hi].astype(F32).reshape(count, 128)
                    after = (before + mix[:, 128 * h : 128 * h + 128]).astype(BF16).astype(F32)
                    x1s[h, lo:hi] = after.reshape(hi - lo, 8, 128).astype(BF16)
                    rows.append(after)
                project(1, rows, lo, hi)
                send_partials(1, first, last)
            residual = remote(
                x1s.at[other, slot_here], xr1, l_send, l_recv, t, z, other
            )
            residual.start()
            lax.fori_loop(1, TP, exit_step_last, 0)
        row8 = lax.broadcasted_iota(jnp.int32, (8, 128), 0)
        live8 = jnp.zeros((8, 128), jnp.int32)
        for s in range(3):
            live8 = jnp.where(row8 // 2 == s, live_ref[s], live8)
        live_rows = (row8 % 2) < live8
        fade8 = jnp.where(low_half[0:6], fade_columns[:, 2 * b : 2 * b + 1], fade_columns[:, 2 * b + 1 : 2 * b + 2])

        all_of(cr.at[b], c_send.at[b], c_recv.at[b]).wait_recv()
        summed[0:40, :] = jnp.sum(cr[b].astype(F32), axis=0)
        square_rows = summed[36:39, :]
        low_squares = square_rows[:, 0:1]
        high_squares = square_rows[:, 64:65]
        token_squares = jnp.concatenate([low_squares, high_squares], axis=0)
        row_scale = lax.rsqrt(token_squares / D + NORM_EPS)
        read, key, value, decay_pre, rate_pre, gate_pre = [
            summed[p * 6 : p * 6 + 6, :] * row_scale for p in range(6)
        ]
        decay = jnp.exp(fade8 - ceil[b : b + 1, :] * jax.nn.sigmoid(decay_pre))
        rate = jax.nn.sigmoid(rate_pre)
        gate = jax.nn.sigmoid(gate_pre)
        removal = key * rate / (head_sum(key * key) + 1e-06)
        spread = head_sum(
            jnp.concatenate(
                [jnp.where(diagonal, value[i : i + 1, :], 0.0) for i in range(6)], axis=0
            )
        )
        memory = [packed[b, s] for s in range(3)]
        readouts = [None] * 6
        spreads = [None] * 6
        for j in range(2):
            removed = head_sum(
                jnp.concatenate(
                    [memory[s] * key[2 * s + j : 2 * s + j + 1, :] for s in range(3)], axis=0
                )
            )
            for s in range(3):
                i = 2 * s + j
                updated = (
                    memory[s] * decay[i : i + 1, :]
                    - removed[64 * s : 64 * s + 64] * removal[i : i + 1, :]
                    + spread[64 * i : 64 * i + 64] * key[i : i + 1, :]
                )
                memory[s] = jnp.where(j < live_ref[s], updated, memory[s])
            read_out = head_sum(
                jnp.concatenate(
                    [memory[s] * read[2 * s + j : 2 * s + j + 1, :] for s in range(3)], axis=0
                )
            )
            for s in range(3):
                here = read_out[64 * s : 64 * s + 64]
                here = here - jnp.sum(here, axis=0, keepdims=True) * (1.0 / 64.0)
                spreads[2 * s + j] = jnp.sum(here * here, axis=0, keepdims=True)
                readouts[2 * s + j] = jnp.sum(
                    jnp.where(diagonal, here, 0.0), axis=0, keepdims=True
                )
        variance = jnp.concatenate(spreads, axis=0) * (1.0 / 64.0)
        centered = jnp.concatenate(readouts, axis=0)
        normed = centered * lax.rsqrt(variance + GROUP_EPS) * resc[b : b + 1, :]
        mixed = jnp.where(live_rows[0:6], normed * gate, 0.0)
        ms[b] = jnp.concatenate([mixed, jnp.zeros((2, 128), F32)], axis=0).astype(BF16)

        if b == 0:
            for g in (2, 1, 0):
                lo, hi, first, last = groups[g]

                def start(to, here, there):
                    remote(
                        ms.at[0], mg.at[there], e_send.at[g], e_recv.at[g], t, to, other
                    ).start()

                column(start, first, last)
            all_of(wall0.at[0:15, :, mine], w_send.at[0], w_recv.at[0]).wait_recv()
            swaps[3].start()
            swaps[2].start()
        else:
            def start_both(to, here, there):
                for core in range(2):
                    remote(
                        ms.at[1], fin.at[c * TP + t], e_send.at[3], e_recv.at[3], z, to, core
                    ).start()

            column(start_both, 1, 8, False)

            @pl.when(t == z)
            def _():
                remote(
                    ms.at[1], fin.at[c * TP + t], e_send.at[3], e_recv.at[3], z, z, other
                ).start()
                fin[c * TP + t] = ms[1]

            @pl.when(t != z)
            def _():
                for core in range(2):
                    remote(
                        ms.at[1], fin.at[c * TP + t], e_send.at[3], e_recv.at[3], z, z, core
                    ).start()

        for s in range(3):
            states[b, s, 0] = memory[s][:, 0:64]
            states[b, s, 1] = memory[s][:, 64:128]

        if b == 0:
            for g, (lo, hi, first, last) in enumerate(groups):
                arriving = mg.at[lo:hi]
                all_of(arriving, e_send.at[g], e_recv.at[g]).wait_recv()

                for up, right in AROUND:
                    remote(
                        mg.at[lo:hi], xw.at[t, lo:hi], f_send.at[g], f_recv.at[g],
                        in_plane(up, right), z, c,
                    ).start()
                xw[t, lo:hi] = mg[lo:hi]

    all_of(wall1.at[0:15], w_send.at[1], w_recv.at[1]).wait_recv()
    residual.wait_recv()

    @pl.when(t == z)
    def _():
        all_of(fin.at[0:31], e_send.at[3], e_recv.at[3]).wait_recv()

    @pl.when(t != z)
    def _():
        all_of(fin, e_send.at[3], e_recv.at[3]).wait_recv()

    heads = jnp.concatenate(
        [
            jnp.concatenate([fin[i].astype(F32), fin[TP + i].astype(F32)], axis=0).astype(BF16)
            for i in range(TP)
        ],
        axis=1,
    )
    mix = jnp.dot(heads, wall1[...].reshape(WIDTH, 128), preferred_element_type=F32)
    here_rows = x1s[c, slot_here].astype(F32)
    there_rows = xr1[...].astype(F32)
    core = jnp.full((8, 128), c, jnp.int32)
    xrows[0:6, :] = (jnp.where(core == 0, there_rows, here_rows) + mix[0:8])[0:6]
    xrows[6:12, :] = (jnp.where(core == 0, here_rows, there_rows) + mix[8:16])[0:6]
    out_ref[...] = xrows[0:12, :].astype(BF16)

    for copy in swaps:
        copy.wait_send()
    residual.wait_send()
    all_of(fin.at[0:7], a_send.at[0], a_recv.at[0]).wait_send()
    all_of(fin, a_send.at[1], a_recv.at[1]).wait_send()
    all_of(wall0.at[0:15, :, mine], w_send.at[0], w_recv.at[0]).wait_send()
    all_of(wall1.at[0:15], w_send.at[1], w_recv.at[1]).wait_send()
    for b in range(2):
        all_of(cr.at[b], c_send.at[b], c_recv.at[b]).wait_send()
    for g, (lo, hi, first, last) in enumerate(groups):
        all_of(mg.at[lo:hi], e_send.at[g], e_recv.at[g]).wait_send()
        all_of(xw.at[0:15, lo:hi], f_send.at[g], f_recv.at[g]).wait_send()

    @pl.when(t == z)
    def _():
        all_of(fin.at[0:31], e_send.at[3], e_recv.at[3]).wait_send()

    @pl.when(t != z)
    def _():
        all_of(fin, e_send.at[3], e_recv.at[3]).wait_send()


def shards(*arrays):
    arrays = arrays[:13] + (jnp.transpose(arrays[13], (0, 2, 1)),)
    arrays = tuple(pltpu.with_memory_space_constraint(a, pltpu.HBM) for a in arrays)
    hbm = pl.BlockSpec(memory_space=pltpu.HBM)
    in_specs = [hbm] * 14
    dma = pltpu.SemaphoreType.DMA
    return pl.pallas_call(
        kernel,
        out_shape=(
            pltpu.VMEM((12, 128), BF16),
            pltpu.VMEM((2, 3, 2, 64, 64), F32),
        ),
        in_specs=in_specs,
        out_specs=(pl.BlockSpec(memory_space=pltpu.VMEM),) * 2,
        scratch_shapes=[
            pltpu.SMEM((3,), jnp.int32),
            pltpu.VMEM((12, 128), BF16),
            pltpu.VMEM((16, 128), F32),
            pltpu.VMEM((2, 8, 128), BF16),
            pltpu.VMEM((2, 2, 128), BF16),
            pltpu.VMEM((2, 256, 768), BF16),
            pltpu.VMEM((16, 128, 256), BF16),
            pltpu.VMEM((16, 128, 128), BF16),
            pltpu.VMEM((2, 128), F32),
            pltpu.VMEM((2, 128), F32),
            pltpu.VMEM((2, 2, 6), F32),
            pltpu.VMEM((2, 3, 2, 64, 64), F32),
            pltpu.VMEM((2, 3, 64, 128), F32),
            pltpu.VMEM((2, 16, 8, 128), BF16),
            pltpu.VMEM((2, 16, 8, 128), BF16),
            pltpu.VMEM((2, 16, 8, 128), BF16),
            pltpu.VMEM((16, 40, 128), F32),
            pltpu.VMEM((2, 16, 40, 128), BF16),
            pltpu.VMEM((2, 16, 40, 128), BF16),
            pltpu.VMEM((40, 128), F32),
            pltpu.VMEM((2, 8, 128), BF16),
            pltpu.VMEM((16, 8, 128), BF16),
            pltpu.VMEM((16, 16, 8, 128), BF16),
            pltpu.VMEM((2, 16, 8, 128), BF16),
            pltpu.VMEM((8, 128), BF16),
            pltpu.VMEM((32, 8, 128), BF16),
            dma((15,)),
            dma((4,)),
            dma((4,)),
            dma((2,)),
            dma((2,)),
            dma((2,)),
            dma((2,)),
            dma((4,)),
            dma((4,)),
            dma((3,)),
            dma((3,)),
            dma((2,)),
            dma((2,)),
            dma,
            dma,
            pltpu.SemaphoreType.REGULAR((2,)),
        ],
        compiler_params=pltpu.CompilerParams(collective_id=0, has_side_effects=True, vmem_limit_bytes=24 * 1024 * 1024),
    )(*arrays)


def solution(mesh):
    in_specs = (
        P("tp", "dp"),
        P("dp"),
        P(None, "dp"),
        P(None, "dp", "tp"),
        P(None, "dp", "tp"),
        P(None, "dp", "tp"),
        P(None, "dp", "tp"),
        P(None, "dp", "tp"),
        P(None, "dp", "tp"),
        P(None, "tp"),
        P(None, "tp"),
        P(None, "tp", "dp"),
        P(None, "dp", "tp", None, None),
        P(None, "dp", "tp"),
    )
    out_specs = (P("tp", "dp"), P(None, "dp", "tp", None, None))
    return jax.shard_map(shards, mesh=mesh, in_specs=in_specs, out_specs=out_specs, check_vma=False)
```

```python
import jax
import jax.numpy as jnp
from jax import lax
from jax.experimental import pallas as pl
from jax.experimental.pallas import tpu as pltpu
from jax.sharding import PartitionSpec as P

D = 4096
NORM_EPS = 1e-06
GROUP_EPS = 0.00064
TP = 16
NZ = 16
NEAR = 4
SIDE = 4
AROUND = sorted(
    ((i, j) for i in range(SIDE) for j in range(SIDE) if i + j > 0),
    key=lambda at: -min(at[0], SIDE - at[0]) - min(at[1], SIDE - at[1]),
)
WIDTH = 2048
F32 = jnp.float32
BF16 = jnp.bfloat16
MESH = pl.DeviceIdType.MESH


def split_two(x):
    hi = x.astype(BF16)
    lo = (x - hi.astype(F32)).astype(BF16)
    return jnp.concatenate([hi, lo], axis=1)


def kernel(
    x_hbm, live_hbm, gain_hbm, wq, wk, wv, wf, wl, we, ceil_hbm, resc_hbm, wo_hbm, mem_hbm, fade_hbm,
    out_ref, states,
    live_ref, xin, xrows, xs, gains, wcat, wall0, wall1, ceil, resc, fade, mem, packed,
    xg, acc, cs, cr, summed, ms, mg, xw, x1s, xr1, fin,
    load_sem, swap_send, swap_recv, a_send, a_recv, c_send, c_recv, e_send, e_recv, f_send, f_recv,
    w_send, w_recv, l_send, l_recv, far_sem,
):
    t = lax.axis_index("tp")
    d = lax.axis_index("dp")
    z = d // 2
    c = d % 2
    other = 1 - c
    away = (t + NZ - z) % NZ
    past_half = away // 9
    slot_here = (1 - past_half) * (2 * away - (away + 15) // 16) + past_half * (32 - 2 * away)

    load_rows = pltpu.make_async_copy(x_hbm, xin, load_sem.at[0])
    load_rows.start()
    barrier = pltpu.get_barrier_semaphore()

    y = t // SIDE
    x = t % SIDE

    def in_plane(up, right):
        return ((y + up) % SIDE) * SIDE + (x + right) % SIDE

    def greet_column(r, carry):
        for to in ((z + r) % NZ, (z + NZ - r) % NZ):
            pl.semaphore_signal(barrier, inc=1, device_id=(t, to * 2 + c), device_id_type=MESH)
        return carry

    for r in range(NEAR, 0, -1):
        greet_column(r, 0)
    for up, right in AROUND:
        for core in range(2):
            pl.semaphore_signal(
                barrier, inc=1, device_id=(in_plane(up, right), z * 2 + core), device_id_type=MESH
            )
    pl.semaphore_signal(barrier, inc=1, device_id=(t, z * 2 + other), device_id_type=MESH)

    mine = pl.ds(pl.multiple_of(c * 128, 128), 128)
    weights = (wq, wk, wv, wf, wl, we)
    loads = [pltpu.make_async_copy(live_hbm, live_ref, load_sem.at[14])]
    for p, w in enumerate(weights):
        loads.append(
            pltpu.make_async_copy(w, wcat.at[:, mine, pl.ds(p * 128, 128)], load_sem.at[1 + p])
        )
    loads.append(pltpu.make_async_copy(wo_hbm.at[0], wall0.at[t, :, mine], load_sem.at[7]))
    loads.append(pltpu.make_async_copy(wo_hbm.at[1], wall1.at[t], load_sem.at[13]))
    loads.append(pltpu.make_async_copy(gain_hbm, gains.at[c], load_sem.at[8]))
    loads.append(pltpu.make_async_copy(ceil_hbm, ceil, load_sem.at[9]))
    loads.append(pltpu.make_async_copy(resc_hbm, resc, load_sem.at[10]))
    loads.append(pltpu.make_async_copy(mem_hbm, mem, load_sem.at[11]))
    loads.append(pltpu.make_async_copy(fade_hbm, fade, load_sem.at[12]))
    for copy in loads:
        copy.start()

    lane = lax.broadcasted_iota(jnp.int32, (8, 128), 1)
    low_half = lane < 64
    row_at = lax.broadcasted_iota(jnp.int32, (256, 128), 0)
    lane_at = lax.broadcasted_iota(jnp.int32, (256, 128), 1)
    ones_block = jnp.where((row_at % 128) // 64 == lane_at // 64, 1.0, 0.0).astype(BF16)
    own_row = lax.broadcasted_iota(jnp.int32, (64, 128), 0)
    own_lane = lax.broadcasted_iota(jnp.int32, (64, 128), 1)
    diagonal = (own_lane % 64) == own_row

    def head_sum(x):
        return jnp.dot(split_two(x), ones_block, preferred_element_type=F32)

    load_rows.wait()
    xrows[...] = jnp.zeros((16, 128), F32)
    xrows[0:12, :] = xin[...].astype(F32)
    first = xrows[0:8, :]
    second = xrows[6:14, :]
    xs[0] = first.astype(BF16)
    xs[1] = second.astype(BF16)
    pl.semaphore_wait(barrier, 2 * (TP - 1) + 1 + 2 * NEAR)

    def remote(src, dst, send, recv, to_t, to_z, to_c):
        return pltpu.make_async_remote_copy(
            src_ref=src, dst_ref=dst, send_sem=send, recv_sem=recv,
            device_id=(to_t, to_z * 2 + to_c), device_id_type=MESH,
        )

    def to_sibling(src, i):
        return remote(src, src, swap_send.at[i], swap_recv.at[i], t, z, other)

    def row_copy(to, core):
        return remote(
            xs.at[core], xg.at[c, slot_here], a_send, a_recv, to, z, core
        )

    for up, right in AROUND:
        row_copy(in_plane(up, right), 0).start()
        row_copy(in_plane(up, right), 1).start()
    row_copy(t, other).start()
    for to in ((z + NEAR) % NZ, (z + NZ - NEAR) % NZ):
        pl.semaphore_signal(far_sem, inc=1, device_id=(t, to * 2 + c), device_id_type=MESH)
    xg[c, slot_here] = xs[c]

    swaps = [
        to_sibling(gains.at[c], 0),
        to_sibling(wcat.at[0, mine, :], 1),
        to_sibling(wcat.at[1, mine, :], 2),
        to_sibling(wall0.at[:, :, mine], 3),
    ]
    for copy in loads:
        copy.wait()
    swaps[0].start()
    swaps[1].start()

    def exit_step(r, carry):
        mine_here = wall0.at[t, :, mine]
        remote(mine_here, mine_here, w_send.at[0], w_recv.at[0], (t + r) % TP, z, c).start()
        return carry

    def exit_step_last(r, carry):
        remote(wall1.at[t], wall1.at[t], w_send.at[1], w_recv.at[1], (t + r) % TP, z, c).start()
        return carry

    for b in range(2):
        for s in range(3):
            packed[b, s] = jnp.concatenate([mem[b, s, 0], mem[b, s, 1]], axis=1)

    fade_columns = jnp.transpose(jnp.concatenate([fade[0], fade[1], jnp.zeros((4, 6), F32)], axis=0))

    def all_of(ref, send, recv):
        return remote(ref, ref, send, recv, t, z, other)

    def column(start, first, last):
        if last == 8:
            start((z + 8) % NZ, 15, 15)

        def step(i, carry):
            dist = min(last, 7) - i
            start((z + dist) % NZ, 2 * dist - 1, 2 * dist)
            start((z + NZ - dist) % NZ, 2 * dist, 2 * dist - 1)
            return carry

        lax.fori_loop(0, min(last, 7) - first + 1, step, 0)

    def project(b, rows, lo, hi):
        count = (hi - lo) * 8
        gained = jnp.concatenate(
            [(rows[h] * gains[h, b : b + 1, :].astype(F32)).astype(BF16) for h in range(2)],
            axis=1,
        )
        squares = jnp.sum(rows[0] * rows[0] + rows[1] * rows[1], axis=1, keepdims=True)
        squares = jnp.broadcast_to(squares, (count, 128)).reshape(hi - lo, 8, 128)
        lower = lax.broadcasted_iota(jnp.int32, (hi - lo, 3, 128), 2) < 64
        acc[lo:hi, 36:40, :] = jnp.zeros((hi - lo, 4, 128), F32)
        acc[lo:hi, 36:39, :] = jnp.where(lower, squares[:, 0:3], squares[:, 3:6])
        for p in range(6):
            part = jnp.dot(
                gained, wcat[b, :, p * 128 : (p + 1) * 128], preferred_element_type=F32
            )
            acc[lo:hi, p * 6 : p * 6 + 6, :] = part.reshape(hi - lo, 8, 128)[:, 0:6]
        cs[b, lo:hi] = acc[lo:hi].astype(BF16)

    def send_partials(b, first, last):
        def start(to, here, there):
            remote(cs.at[b, here], cr.at[b, z], c_send.at[b], c_recv.at[b], t, to, c).start()

        column(start, first, last)

    groups = ((0, 3, 1, 1), (3, 7, 2, 3), (7, 11, 4, 5), (11, 15, 6, 7), (15, 16, 8, 8))
    for b in range(2):
        if b == 0:
            swaps[0].wait_recv()
            swaps[1].wait_recv()
            all_of(fin.at[0:31], a_send, a_recv).wait_recv()
            rows = [xg[h].astype(F32).reshape(128, 128) for h in range(2)]
            project(0, rows, 0, 16)
            pl.semaphore_wait(far_sem, 2)
            send_partials(0, 1, 8)
            lax.fori_loop(1, TP, exit_step, 0)
        else:
            swaps[2].wait_recv()
            swaps[3].wait_recv()
            for g, (lo, hi, first, last) in enumerate(groups):
                count = (hi - lo) * 8
                all_of(xw.at[0:15, lo:hi], f_send.at[g], f_recv.at[g]).wait_recv()
                heads = jnp.concatenate(
                    [xw[i, lo:hi].astype(F32).reshape(count, 128).astype(BF16) for i in range(TP)],
                    axis=1,
                )
                mix = jnp.dot(
                    heads, wall0[...].reshape(WIDTH, 256), preferred_element_type=F32
                )
                rows = []
                for h in range(2):
                    before = xg[h, lo:hi].astype(F32).reshape(count, 128)
                    after = (before + mix[:, 128 * h : 128 * h + 128]).astype(BF16).astype(F32)
                    x1s[h, lo:hi] = after.reshape(hi - lo, 8, 128).astype(BF16)
                    rows.append(after)
                project(1, rows, lo, hi)
                send_partials(1, first, last)
            residual = remote(
                x1s.at[other, slot_here], xr1, l_send, l_recv, t, z, other
            )
            residual.start()
            lax.fori_loop(1, TP, exit_step_last, 0)
        own = cs[b, 0]
        cr[b, z] = own

        row8 = lax.broadcasted_iota(jnp.int32, (8, 128), 0)
        live8 = jnp.zeros((8, 128), jnp.int32)
        for s in range(3):
            live8 = jnp.where(row8 // 2 == s, live_ref[s], live8)
        live_rows = (row8 % 2) < live8
        fade8 = jnp.where(low_half[0:6], fade_columns[:, 2 * b : 2 * b + 1], fade_columns[:, 2 * b + 1 : 2 * b + 2])

        all_of(cr.at[b, 0:15], c_send.at[b], c_recv.at[b]).wait_recv()
        summed[0:40, :] = jnp.sum(cr[b].astype(F32), axis=0)
        square_rows = summed[36:39, :]
        low_squares = square_rows[:, 0:1]
        high_squares = square_rows[:, 64:65]
        token_squares = jnp.concatenate([low_squares, high_squares], axis=0)
        row_scale = lax.rsqrt(token_squares / D + NORM_EPS)
        read, key, value, decay_pre, rate_pre, gate_pre = [
            summed[p * 6 : p * 6 + 6, :] * row_scale for p in range(6)
        ]
        decay = jnp.exp(fade8 - ceil[b : b + 1, :] * jax.nn.sigmoid(decay_pre))
        rate = jax.nn.sigmoid(rate_pre)
        gate = jax.nn.sigmoid(gate_pre)
        removal = key * rate / (head_sum(key * key) + 1e-06)
        spread = head_sum(
            jnp.concatenate(
                [jnp.where(diagonal, value[i : i + 1, :], 0.0) for i in range(6)], axis=0
            )
        )
        memory = [packed[b, s] for s in range(3)]
        readouts = [None] * 6
        spreads = [None] * 6
        for j in range(2):
            removed = head_sum(
                jnp.concatenate(
                    [memory[s] * key[2 * s + j : 2 * s + j + 1, :] for s in range(3)], axis=0
                )
            )
            for s in range(3):
                i = 2 * s + j
                updated = (
                    memory[s] * decay[i : i + 1, :]
                    - removed[64 * s : 64 * s + 64] * removal[i : i + 1, :]
                    + spread[64 * i : 64 * i + 64] * key[i : i + 1, :]
                )
                memory[s] = jnp.where(j < live_ref[s], updated, memory[s])
            read_out = head_sum(
                jnp.concatenate(
                    [memory[s] * read[2 * s + j : 2 * s + j + 1, :] for s in range(3)], axis=0
                )
            )
            for s in range(3):
                here = read_out[64 * s : 64 * s + 64]
                here = here - jnp.sum(here, axis=0, keepdims=True) * (1.0 / 64.0)
                spreads[2 * s + j] = jnp.sum(here * here, axis=0, keepdims=True)
                readouts[2 * s + j] = jnp.sum(
                    jnp.where(diagonal, here, 0.0), axis=0, keepdims=True
                )
        variance = jnp.concatenate(spreads, axis=0) * (1.0 / 64.0)
        centered = jnp.concatenate(readouts, axis=0)
        normed = centered * lax.rsqrt(variance + GROUP_EPS) * resc[b : b + 1, :]
        mixed = jnp.where(live_rows[0:6], normed * gate, 0.0)
        ms[b] = jnp.concatenate([mixed, jnp.zeros((2, 128), F32)], axis=0).astype(BF16)

        if b == 0:
            for g in (4, 3, 2, 1, 0):
                lo, hi, first, last = groups[g]

                def start(to, here, there):
                    remote(
                        ms.at[0], mg.at[there], e_send.at[g], e_recv.at[g], t, to, c
                    ).start()

                column(start, first, last)
            mg[0] = ms[0]
            all_of(wall0.at[0:15, :, mine], w_send.at[0], w_recv.at[0]).wait_recv()
            swaps[3].start()
            swaps[2].start()
        else:
            def start_both(to, here, there):
                for core in range(2):
                    remote(
                        ms.at[1], fin.at[c * TP + t], e_send.at[5], e_recv.at[5], z, to, core
                    ).start()

            column(start_both, 1, 8)

            @pl.when(t == z)
            def _():
                remote(
                    ms.at[1], fin.at[c * TP + t], e_send.at[5], e_recv.at[5], z, z, other
                ).start()
                fin[c * TP + t] = ms[1]

            @pl.when(t != z)
            def _():
                for core in range(2):
                    remote(
                        ms.at[1], fin.at[c * TP + t], e_send.at[5], e_recv.at[5], z, z, core
                    ).start()

        for s in range(3):
            states[b, s, 0] = memory[s][:, 0:64]
            states[b, s, 1] = memory[s][:, 64:128]

        if b == 0:
            for g, (lo, hi, first, last) in enumerate(groups):
                arriving = mg.at[max(lo, 1) : hi]
                all_of(arriving, e_send.at[g], e_recv.at[g]).wait_recv()

                for up, right in AROUND:
                    remote(
                        mg.at[lo:hi], xw.at[t, lo:hi], f_send.at[g], f_recv.at[g],
                        in_plane(up, right), z, c,
                    ).start()
                xw[t, lo:hi] = mg[lo:hi]

    all_of(wall1.at[0:15], w_send.at[1], w_recv.at[1]).wait_recv()
    residual.wait_recv()

    @pl.when(t == z)
    def _():
        all_of(fin.at[0:31], e_send.at[5], e_recv.at[5]).wait_recv()

    @pl.when(t != z)
    def _():
        all_of(fin, e_send.at[5], e_recv.at[5]).wait_recv()

    heads = jnp.concatenate(
        [
            jnp.concatenate([fin[i].astype(F32), fin[TP + i].astype(F32)], axis=0).astype(BF16)
            for i in range(TP)
        ],
        axis=1,
    )
    mix = jnp.dot(heads, wall1[...].reshape(WIDTH, 128), preferred_element_type=F32)
    here_rows = x1s[c, slot_here].astype(F32)
    there_rows = xr1[...].astype(F32)
    core = jnp.full((8, 128), c, jnp.int32)
    xrows[0:6, :] = (jnp.where(core == 0, here_rows, there_rows) + mix[0:8])[0:6]
    xrows[6:12, :] = (jnp.where(core == 0, there_rows, here_rows) + mix[8:16])[0:6]
    out_ref[...] = xrows[0:12, :].astype(BF16)

    for copy in swaps:
        copy.wait_send()
    residual.wait_send()
    all_of(fin.at[0:31], a_send, a_recv).wait_send()
    all_of(wall0.at[0:15, :, mine], w_send.at[0], w_recv.at[0]).wait_send()
    all_of(wall1.at[0:15], w_send.at[1], w_recv.at[1]).wait_send()
    for b in range(2):
        all_of(cr.at[b, 0:15], c_send.at[b], c_recv.at[b]).wait_send()
    for g, (lo, hi, first, last) in enumerate(groups):
        all_of(mg.at[max(lo, 1) : hi], e_send.at[g], e_recv.at[g]).wait_send()
        all_of(xw.at[0:15, lo:hi], f_send.at[g], f_recv.at[g]).wait_send()

    @pl.when(t == z)
    def _():
        all_of(fin.at[0:31], e_send.at[5], e_recv.at[5]).wait_send()

    @pl.when(t != z)
    def _():
        all_of(fin, e_send.at[5], e_recv.at[5]).wait_send()


def store_results(rows_ref, states_ref, rows_out, states_out, sem):
    copies = [
        pltpu.make_async_copy(states_ref, states_out, sem.at[0]),
        pltpu.make_async_copy(rows_ref, rows_out, sem.at[1]),
    ]
    for copy in copies:
        copy.start()
    for copy in copies:
        copy.wait()


def shards(*arrays):
    arrays = arrays[:13] + (jnp.transpose(arrays[13], (0, 2, 1)),)
    arrays = tuple(pltpu.with_memory_space_constraint(a, pltpu.HBM) for a in arrays)
    hbm = pl.BlockSpec(memory_space=pltpu.HBM)
    in_specs = [hbm] * 14
    dma = pltpu.SemaphoreType.DMA
    results = pl.pallas_call(
        kernel,
        out_shape=(
            pltpu.VMEM((12, 128), BF16),
            pltpu.VMEM((2, 3, 2, 64, 64), F32),
        ),
        in_specs=in_specs,
        out_specs=(pl.BlockSpec(memory_space=pltpu.VMEM),) * 2,
        scratch_shapes=[
            pltpu.SMEM((3,), jnp.int32),
            pltpu.VMEM((12, 128), BF16),
            pltpu.VMEM((16, 128), F32),
            pltpu.VMEM((2, 8, 128), BF16),
            pltpu.VMEM((2, 2, 128), BF16),
            pltpu.VMEM((2, 256, 768), BF16),
            pltpu.VMEM((16, 128, 256), BF16),
            pltpu.VMEM((16, 128, 128), BF16),
            pltpu.VMEM((2, 128), F32),
            pltpu.VMEM((2, 128), F32),
            pltpu.VMEM((2, 2, 6), F32),
            pltpu.VMEM((2, 3, 2, 64, 64), F32),
            pltpu.VMEM((2, 3, 64, 128), F32),
            pltpu.VMEM((2, 16, 8, 128), BF16),
            pltpu.VMEM((16, 40, 128), F32),
            pltpu.VMEM((2, 16, 40, 128), BF16),
            pltpu.VMEM((2, 16, 40, 128), BF16),
            pltpu.VMEM((40, 128), F32),
            pltpu.VMEM((2, 8, 128), BF16),
            pltpu.VMEM((16, 8, 128), BF16),
            pltpu.VMEM((16, 16, 8, 128), BF16),
            pltpu.VMEM((2, 16, 8, 128), BF16),
            pltpu.VMEM((8, 128), BF16),
            pltpu.VMEM((32, 8, 128), BF16),
            dma((15,)),
            dma((4,)),
            dma((4,)),
            dma,
            dma,
            dma((2,)),
            dma((2,)),
            dma((6,)),
            dma((6,)),
            dma((5,)),
            dma((5,)),
            dma((2,)),
            dma((2,)),
            dma,
            dma,
            pltpu.SemaphoreType.REGULAR,
        ],
        compiler_params=pltpu.CompilerParams(collective_id=0, has_side_effects=True, vmem_limit_bytes=24 * 1024 * 1024),
    )(*arrays)
    return pl.pallas_call(
        store_results,
        out_shape=(
            jax.ShapeDtypeStruct((12, 128), BF16),
            jax.ShapeDtypeStruct((2, 3, 2, 64, 64), F32),
        ),
        in_specs=[pl.BlockSpec(memory_space=pltpu.VMEM)] * 2,
        out_specs=(hbm, hbm),
        scratch_shapes=[dma((2,))],
        compiler_params=pltpu.CompilerParams(vmem_limit_bytes=1024 * 1024),
    )(*results)


def solution(mesh):
    in_specs = (
        P("tp", "dp"),
        P("dp"),
        P(None, "dp"),
        P(None, "dp", "tp"),
        P(None, "dp", "tp"),
        P(None, "dp", "tp"),
        P(None, "dp", "tp"),
        P(None, "dp", "tp"),
        P(None, "dp", "tp"),
        P(None, "tp"),
        P(None, "tp"),
        P(None, "tp", "dp"),
        P(None, "dp", "tp", None, None),
        P(None, "dp", "tp"),
    )
    out_specs = (P("tp", "dp"), P(None, "dp", "tp", None, None))
    return jax.shard_map(shards, mesh=mesh, in_specs=in_specs, out_specs=out_specs, check_vma=False)
```

```python
import jax
import jax.numpy as jnp
from jax import lax
from jax.experimental import pallas as pl
from jax.experimental.pallas import tpu as pltpu
from jax.sharding import PartitionSpec as P

D = 4096
NORM_EPS = 1e-06
GROUP_EPS = 0.00064
TP = 16
NZ = 16
NEAR = 4
SENT = 38
SIDE = 4
AROUND = sorted(
    ((i, j) for i in range(SIDE) for j in range(SIDE) if i + j > 0),
    key=lambda at: -min(at[0], SIDE - at[0]) - min(at[1], SIDE - at[1]),
)
WIDTH = 2048
F32 = jnp.float32
BF16 = jnp.bfloat16
MESH = pl.DeviceIdType.MESH


def split_two(x):
    hi = x.astype(BF16)
    lo = (x - hi.astype(F32)).astype(BF16)
    return jnp.concatenate([hi, lo], axis=1)


def kernel(
    x_hbm, live_hbm, gain_hbm, wq, wk, wv, wf, wl, we, ceil_hbm, resc_hbm, wo_hbm, mem_hbm, fade_hbm,
    out_ref, states,
    live_ref, xin, xrows, xs, gains, wcat, wall0, wall1, ceil, resc, fade, mem, packed,
    xg, acc, cs, cr, summed, ms, mg, xw, x1s, xr1, fin,
    load_sem, swap_send, swap_recv, a_send, a_recv, c_send, c_recv, e_send, e_recv, f_send, f_recv,
    w_send, w_recv, l_send, l_recv, far_sem,
):
    t = lax.axis_index("tp")
    d = lax.axis_index("dp")
    z = d // 2
    c = d % 2
    other = 1 - c
    away = (t + NZ - z) % NZ
    past_half = away // 9
    slot_here = (1 - past_half) * (2 * away - (away + 15) // 16) + past_half * (32 - 2 * away)

    load_rows = pltpu.make_async_copy(x_hbm, xin, load_sem.at[0])
    load_rows.start()
    barrier = pltpu.get_barrier_semaphore()

    y = t // SIDE
    x = t % SIDE

    def in_plane(up, right):
        return ((y + up) % SIDE) * SIDE + (x + right) % SIDE

    def greet_column(r, carry):
        for to in ((z + r) % NZ, (z + NZ - r) % NZ):
            pl.semaphore_signal(barrier, inc=1, device_id=(t, to * 2 + c), device_id_type=MESH)
        return carry

    for r in range(NEAR, 0, -1):
        greet_column(r, 0)
    for up, right in AROUND:
        for core in range(2):
            pl.semaphore_signal(
                barrier, inc=1, device_id=(in_plane(up, right), z * 2 + core), device_id_type=MESH
            )
    pl.semaphore_signal(barrier, inc=1, device_id=(t, z * 2 + other), device_id_type=MESH)

    mine = pl.ds(pl.multiple_of(c * 128, 128), 128)
    weights = (wq, wk, wv, wf, wl, we)
    loads = [pltpu.make_async_copy(live_hbm, live_ref, load_sem.at[14])]
    for p, w in enumerate(weights):
        loads.append(
            pltpu.make_async_copy(w, wcat.at[:, mine, pl.ds(p * 128, 128)], load_sem.at[1 + p])
        )
    loads.append(pltpu.make_async_copy(wo_hbm.at[0], wall0.at[t, :, mine], load_sem.at[7]))
    loads.append(pltpu.make_async_copy(wo_hbm.at[1], wall1.at[t], load_sem.at[13]))
    loads.append(pltpu.make_async_copy(gain_hbm, gains.at[c], load_sem.at[8]))
    loads.append(pltpu.make_async_copy(ceil_hbm, ceil, load_sem.at[9]))
    loads.append(pltpu.make_async_copy(resc_hbm, resc, load_sem.at[10]))
    loads.append(pltpu.make_async_copy(mem_hbm, mem, load_sem.at[11]))
    loads.append(pltpu.make_async_copy(fade_hbm, fade, load_sem.at[12]))
    for copy in loads:
        copy.start()

    lane = lax.broadcasted_iota(jnp.int32, (8, 128), 1)
    low_half = lane < 64
    row_at = lax.broadcasted_iota(jnp.int32, (256, 128), 0)
    lane_at = lax.broadcasted_iota(jnp.int32, (256, 128), 1)
    ones_block = jnp.where((row_at % 128) // 64 == lane_at // 64, 1.0, 0.0).astype(BF16)
    own_row = lax.broadcasted_iota(jnp.int32, (64, 128), 0)
    own_lane = lax.broadcasted_iota(jnp.int32, (64, 128), 1)
    diagonal = (own_lane % 64) == own_row

    def head_sum(x):
        return jnp.dot(split_two(x), ones_block, preferred_element_type=F32)

    load_rows.wait()
    xrows[...] = jnp.zeros((16, 128), F32)
    xrows[0:12, :] = xin[...].astype(F32)
    first = xrows[0:8, :]
    second = xrows[6:14, :]
    xs[0] = first.astype(BF16)
    xs[1] = second.astype(BF16)
    pl.semaphore_wait(barrier, 2 * (TP - 1) + 1 + 2 * NEAR)

    def remote(src, dst, send, recv, to_t, to_z, to_c):
        return pltpu.make_async_remote_copy(
            src_ref=src, dst_ref=dst, send_sem=send, recv_sem=recv,
            device_id=(to_t, to_z * 2 + to_c), device_id_type=MESH,
        )

    def to_sibling(src, i):
        return remote(src, src, swap_send.at[i], swap_recv.at[i], t, z, other)

    def row_copy(to, core):
        return remote(
            xs.at[core], xg.at[c, slot_here], a_send, a_recv, to, z, core
        )

    for up, right in AROUND:
        row_copy(in_plane(up, right), 0).start()
        row_copy(in_plane(up, right), 1).start()
    row_copy(t, other).start()
    for to in ((z + NEAR) % NZ, (z + NZ - NEAR) % NZ):
        pl.semaphore_signal(far_sem, inc=1, device_id=(t, to * 2 + c), device_id_type=MESH)
    xg[c, slot_here] = xs[c]

    swaps = [
        to_sibling(gains.at[c], 0),
        to_sibling(wcat.at[0, mine, :], 1),
        to_sibling(wcat.at[1, mine, :], 2),
        to_sibling(wall0.at[:, :, mine], 3),
    ]
    for copy in loads[1:7] + loads[9:10]:
        copy.wait()
    swaps[0].start()
    swaps[1].start()
    for copy in loads[0:1] + loads[7:9] + loads[10:]:
        copy.wait()

    def exit_step(r, carry):
        mine_here = wall0.at[t, :, mine]
        remote(mine_here, mine_here, w_send.at[0], w_recv.at[0], (t + r) % TP, z, c).start()
        return carry

    def exit_step_last(r, carry):
        remote(wall1.at[t], wall1.at[t], w_send.at[1], w_recv.at[1], (t + r) % TP, z, c).start()
        return carry

    for b in range(2):
        for s in range(3):
            packed[b, s] = jnp.concatenate([mem[b, s, 0], mem[b, s, 1]], axis=1)

    fade_columns = jnp.transpose(jnp.concatenate([fade[0], fade[1], jnp.zeros((4, 6), F32)], axis=0))

    def all_of(ref, send, recv):
        return remote(ref, ref, send, recv, t, z, other)

    def column(start, first, last):
        if last == 8:
            start((z + 8) % NZ, 15, 15)

        def step(i, carry):
            dist = min(last, 7) - i
            start((z + dist) % NZ, 2 * dist - 1, 2 * dist)
            start((z + NZ - dist) % NZ, 2 * dist, 2 * dist - 1)
            return carry

        lax.fori_loop(0, min(last, 7) - first + 1, step, 0)

    def project(b, rows, lo, hi):
        count = (hi - lo) * 8
        gained = jnp.concatenate(
            [(rows[h] * gains[h, b : b + 1, :].astype(F32)).astype(BF16) for h in range(2)],
            axis=1,
        )
        squares = jnp.sum(rows[0] * rows[0] + rows[1] * rows[1], axis=1, keepdims=True)
        squares = jnp.broadcast_to(squares, (count, 128)).reshape(hi - lo, 8, 128)
        token_at = lax.broadcasted_iota(jnp.int32, (hi - lo, 8, 128), 1)
        place_at = lax.broadcasted_iota(jnp.int32, (hi - lo, 8, 128), 2) // 16
        line = jnp.sum(jnp.where(token_at == place_at, squares, 0.0), axis=1, keepdims=True)
        rounded = line.astype(BF16).astype(F32)
        acc[lo:hi, 36:40, :] = jnp.zeros((hi - lo, 4, 128), F32)
        acc[lo:hi, 36:37, :] = rounded
        acc[lo:hi, 37:38, :] = line - rounded
        for p in range(6):
            part = jnp.dot(
                gained, wcat[b, :, p * 128 : (p + 1) * 128], preferred_element_type=F32
            )
            acc[lo:hi, p * 6 : p * 6 + 6, :] = part.reshape(hi - lo, 8, 128)[:, 0:6]
        cs[b, lo:hi] = acc[lo:hi].astype(BF16)

    def send_partials(b, first, last):
        def start(to, here, there):
            remote(cs.at[b, here, 0:SENT], cr.at[b, z, 0:SENT], c_send.at[b], c_recv.at[b], t, to, c).start()

        column(start, first, last)

    groups = ((0, 3, 1, 1), (3, 7, 2, 3), (7, 11, 4, 5), (11, 15, 6, 7), (15, 16, 8, 8))
    for b in range(2):
        if b == 0:
            swaps[0].wait_recv()
            swaps[1].wait_recv()
            all_of(fin.at[0:31], a_send, a_recv).wait_recv()
            rows = [xg[h].astype(F32).reshape(128, 128) for h in range(2)]
            project(0, rows, 0, 16)
            pl.semaphore_wait(far_sem, 2)
            send_partials(0, 1, 8)
            lax.fori_loop(1, TP, exit_step, 0)
        else:
            swaps[2].wait_recv()
            swaps[3].wait_recv()
            for g, (lo, hi, first, last) in enumerate(groups):
                count = (hi - lo) * 8
                all_of(xw.at[0:15, lo:hi], f_send.at[g], f_recv.at[g]).wait_recv()
                heads = jnp.concatenate(
                    [xw[i, lo:hi].astype(F32).reshape(count, 128).astype(BF16) for i in range(TP)],
                    axis=1,
                )
                mix = jnp.dot(
                    heads, wall0[...].reshape(WIDTH, 256), preferred_element_type=F32
                )
                rows = []
                for h in range(2):
                    before = xg[h, lo:hi].astype(F32).reshape(count, 128)
                    after = (before + mix[:, 128 * h : 128 * h + 128]).astype(BF16).astype(F32)
                    x1s[h, lo:hi] = after.reshape(hi - lo, 8, 128).astype(BF16)
                    rows.append(after)
                project(1, rows, lo, hi)
                send_partials(1, first, last)
            residual = remote(
                x1s.at[other, slot_here], xr1, l_send, l_recv, t, z, other
            )
            residual.start()
            lax.fori_loop(1, TP, exit_step_last, 0)
        own = cs[b, 0]
        cr[b, z] = own

        row8 = lax.broadcasted_iota(jnp.int32, (8, 128), 0)
        live8 = jnp.zeros((8, 128), jnp.int32)
        for s in range(3):
            live8 = jnp.where(row8 // 2 == s, live_ref[s], live8)
        live_rows = (row8 % 2) < live8
        fade8 = jnp.where(low_half[0:6], fade_columns[:, 2 * b : 2 * b + 1], fade_columns[:, 2 * b + 1 : 2 * b + 2])

        all_of(cr.at[b, 0:15, 0:SENT], c_send.at[b], c_recv.at[b]).wait_recv()
        summed[0:40, :] = jnp.sum(cr[b].astype(F32), axis=0)
        line = summed[36:37, :] + summed[37:38, :]
        token_squares = jnp.sum(
            jnp.where(row8[0:6] == lane[0:6] // 16, line, 0.0), axis=1, keepdims=True
        ) * (1.0 / 16.0)
        row_scale = lax.rsqrt(token_squares / D + NORM_EPS)
        read, key, value, decay_pre, rate_pre, gate_pre = [
            summed[p * 6 : p * 6 + 6, :] * row_scale for p in range(6)
        ]
        decay = jnp.exp(fade8 - ceil[b : b + 1, :] * jax.nn.sigmoid(decay_pre))
        rate = jax.nn.sigmoid(rate_pre)
        gate = jax.nn.sigmoid(gate_pre)
        removal = key * rate / (head_sum(key * key) + 1e-06)
        spread = head_sum(
            jnp.concatenate(
                [jnp.where(diagonal, value[i : i + 1, :], 0.0) for i in range(6)], axis=0
            )
        )
        memory = [packed[b, s] for s in range(3)]
        readouts = [None] * 6
        spreads = [None] * 6
        for j in range(2):
            removed = head_sum(
                jnp.concatenate(
                    [memory[s] * key[2 * s + j : 2 * s + j + 1, :] for s in range(3)], axis=0
                )
            )
            for s in range(3):
                i = 2 * s + j
                updated = (
                    memory[s] * decay[i : i + 1, :]
                    - removed[64 * s : 64 * s + 64] * removal[i : i + 1, :]
                    + spread[64 * i : 64 * i + 64] * key[i : i + 1, :]
                )
                memory[s] = jnp.where(j < live_ref[s], updated, memory[s])
            read_out = head_sum(
                jnp.concatenate(
                    [memory[s] * read[2 * s + j : 2 * s + j + 1, :] for s in range(3)], axis=0
                )
            )
            for s in range(3):
                here = read_out[64 * s : 64 * s + 64]
                here = here - jnp.sum(here, axis=0, keepdims=True) * (1.0 / 64.0)
                spreads[2 * s + j] = jnp.sum(here * here, axis=0, keepdims=True)
                readouts[2 * s + j] = jnp.sum(
                    jnp.where(diagonal, here, 0.0), axis=0, keepdims=True
                )
        variance = jnp.concatenate(spreads, axis=0) * (1.0 / 64.0)
        centered = jnp.concatenate(readouts, axis=0)
        normed = centered * lax.rsqrt(variance + GROUP_EPS) * resc[b : b + 1, :]
        mixed = jnp.where(live_rows[0:6], normed * gate, 0.0)
        ms[b] = jnp.concatenate([mixed, jnp.zeros((2, 128), F32)], axis=0).astype(BF16)

        if b == 0:
            for g in (4, 3, 2, 1, 0):
                lo, hi, first, last = groups[g]

                def start(to, here, there):
                    remote(
                        ms.at[0], mg.at[there], e_send.at[g], e_recv.at[g], t, to, c
                    ).start()

                column(start, first, last)
            mg[0] = ms[0]
            all_of(wall0.at[0:15, :, mine], w_send.at[0], w_recv.at[0]).wait_recv()
            swaps[3].start()
            swaps[2].start()
        else:
            def start_both(to, here, there):
                for core in range(2):
                    remote(
                        ms.at[1], fin.at[c * TP + t], e_send.at[5], e_recv.at[5], z, to, core
                    ).start()

            column(start_both, 1, 8)

            @pl.when(t == z)
            def _():
                remote(
                    ms.at[1], fin.at[c * TP + t], e_send.at[5], e_recv.at[5], z, z, other
                ).start()
                fin[c * TP + t] = ms[1]

            @pl.when(t != z)
            def _():
                for core in range(2):
                    remote(
                        ms.at[1], fin.at[c * TP + t], e_send.at[5], e_recv.at[5], z, z, core
                    ).start()

        for s in range(3):
            states[b, s, 0] = memory[s][:, 0:64]
            states[b, s, 1] = memory[s][:, 64:128]

        if b == 0:
            for g, (lo, hi, first, last) in enumerate(groups):
                arriving = mg.at[max(lo, 1) : hi]
                all_of(arriving, e_send.at[g], e_recv.at[g]).wait_recv()

                for up, right in AROUND:
                    remote(
                        mg.at[lo:hi], xw.at[t, lo:hi], f_send.at[g], f_recv.at[g],
                        in_plane(up, right), z, c,
                    ).start()
                xw[t, lo:hi] = mg[lo:hi]

    all_of(wall1.at[0:15], w_send.at[1], w_recv.at[1]).wait_recv()
    residual.wait_recv()

    @pl.when(t == z)
    def _():
        all_of(fin.at[0:31], e_send.at[5], e_recv.at[5]).wait_recv()

    @pl.when(t != z)
    def _():
        all_of(fin, e_send.at[5], e_recv.at[5]).wait_recv()

    heads = jnp.concatenate(
        [
            jnp.concatenate([fin[i].astype(F32), fin[TP + i].astype(F32)], axis=0).astype(BF16)
            for i in range(TP)
        ],
        axis=1,
    )
    mix = jnp.dot(heads, wall1[...].reshape(WIDTH, 128), preferred_element_type=F32)
    here_rows = x1s[c, slot_here].astype(F32)
    there_rows = xr1[...].astype(F32)
    core = jnp.full((8, 128), c, jnp.int32)
    xrows[0:6, :] = (jnp.where(core == 0, here_rows, there_rows) + mix[0:8])[0:6]
    xrows[6:12, :] = (jnp.where(core == 0, there_rows, here_rows) + mix[8:16])[0:6]
    out_ref[...] = xrows[0:12, :].astype(BF16)

    for copy in swaps:
        copy.wait_send()
    residual.wait_send()
    all_of(fin.at[0:31], a_send, a_recv).wait_send()
    all_of(wall0.at[0:15, :, mine], w_send.at[0], w_recv.at[0]).wait_send()
    all_of(wall1.at[0:15], w_send.at[1], w_recv.at[1]).wait_send()
    for b in range(2):
        all_of(cr.at[b, 0:15, 0:SENT], c_send.at[b], c_recv.at[b]).wait_send()
    for g, (lo, hi, first, last) in enumerate(groups):
        all_of(mg.at[max(lo, 1) : hi], e_send.at[g], e_recv.at[g]).wait_send()
        all_of(xw.at[0:15, lo:hi], f_send.at[g], f_recv.at[g]).wait_send()

    @pl.when(t == z)
    def _():
        all_of(fin.at[0:31], e_send.at[5], e_recv.at[5]).wait_send()

    @pl.when(t != z)
    def _():
        all_of(fin, e_send.at[5], e_recv.at[5]).wait_send()


def store_results(rows_ref, states_ref, rows_out, states_out, sem):
    copies = [
        pltpu.make_async_copy(states_ref, states_out, sem.at[0]),
        pltpu.make_async_copy(rows_ref, rows_out, sem.at[1]),
    ]
    for copy in copies:
        copy.start()
    for copy in copies:
        copy.wait()


def shards(*arrays):
    arrays = arrays[:13] + (jnp.transpose(arrays[13], (0, 2, 1)),)
    arrays = tuple(pltpu.with_memory_space_constraint(a, pltpu.HBM) for a in arrays)
    hbm = pl.BlockSpec(memory_space=pltpu.HBM)
    in_specs = [hbm] * 14
    dma = pltpu.SemaphoreType.DMA
    results = pl.pallas_call(
        kernel,
        out_shape=(
            pltpu.VMEM((12, 128), BF16),
            pltpu.VMEM((2, 3, 2, 64, 64), F32),
        ),
        in_specs=in_specs,
        out_specs=(pl.BlockSpec(memory_space=pltpu.VMEM),) * 2,
        scratch_shapes=[
            pltpu.SMEM((3,), jnp.int32),
            pltpu.VMEM((12, 128), BF16),
            pltpu.VMEM((16, 128), F32),
            pltpu.VMEM((2, 8, 128), BF16),
            pltpu.VMEM((2, 2, 128), BF16),
            pltpu.VMEM((2, 256, 768), BF16),
            pltpu.VMEM((16, 128, 256), BF16),
            pltpu.VMEM((16, 128, 128), BF16),
            pltpu.VMEM((2, 128), F32),
            pltpu.VMEM((2, 128), F32),
            pltpu.VMEM((2, 2, 6), F32),
            pltpu.VMEM((2, 3, 2, 64, 64), F32),
            pltpu.VMEM((2, 3, 64, 128), F32),
            pltpu.VMEM((2, 16, 8, 128), BF16),
            pltpu.VMEM((16, 40, 128), F32),
            pltpu.VMEM((2, 16, 40, 128), BF16),
            pltpu.VMEM((2, 16, 40, 128), BF16),
            pltpu.VMEM((40, 128), F32),
            pltpu.VMEM((2, 8, 128), BF16),
            pltpu.VMEM((16, 8, 128), BF16),
            pltpu.VMEM((16, 16, 8, 128), BF16),
            pltpu.VMEM((2, 16, 8, 128), BF16),
            pltpu.VMEM((8, 128), BF16),
            pltpu.VMEM((32, 8, 128), BF16),
            dma((15,)),
            dma((4,)),
            dma((4,)),
            dma,
            dma,
            dma((2,)),
            dma((2,)),
            dma((6,)),
            dma((6,)),
            dma((5,)),
            dma((5,)),
            dma((2,)),
            dma((2,)),
            dma,
            dma,
            pltpu.SemaphoreType.REGULAR,
        ],
        compiler_params=pltpu.CompilerParams(collective_id=0, has_side_effects=True, vmem_limit_bytes=24 * 1024 * 1024),
    )(*arrays)
    return pl.pallas_call(
        store_results,
        out_shape=(
            jax.ShapeDtypeStruct((12, 128), BF16),
            jax.ShapeDtypeStruct((2, 3, 2, 64, 64), F32),
        ),
        in_specs=[pl.BlockSpec(memory_space=pltpu.VMEM)] * 2,
        out_specs=(hbm, hbm),
        scratch_shapes=[dma((2,))],
        compiler_params=pltpu.CompilerParams(vmem_limit_bytes=1024 * 1024),
    )(*results)


def solution(mesh):
    in_specs = (
        P("tp", "dp"),
        P("dp"),
        P(None, "dp"),
        P(None, "dp", "tp"),
        P(None, "dp", "tp"),
        P(None, "dp", "tp"),
        P(None, "dp", "tp"),
        P(None, "dp", "tp"),
        P(None, "dp", "tp"),
        P(None, "tp"),
        P(None, "tp"),
        P(None, "tp", "dp"),
        P(None, "dp", "tp", None, None),
        P(None, "dp", "tp"),
    )
    out_specs = (P("tp", "dp"), P(None, "dp", "tp", None, None))
    return jax.shard_map(shards, mesh=mesh, in_specs=in_specs, out_specs=out_specs, check_vma=False)
```

```python
import jax
import jax.numpy as jnp
from jax import lax
from jax.experimental import pallas as pl
from jax.experimental.pallas import tpu as pltpu
from jax.sharding import PartitionSpec as P

D = 4096
NORM_EPS = 1e-06
GROUP_EPS = 0.00064
TP = 16
NZ = 16
NEAR = 4
SENT = 38
SIDE = 4
AROUND = sorted(
    ((i, j) for i in range(SIDE) for j in range(SIDE) if i + j > 0),
    key=lambda at: -min(at[0], SIDE - at[0]) - min(at[1], SIDE - at[1]),
)
WIDTH = 2048
F32 = jnp.float32
BF16 = jnp.bfloat16
MESH = pl.DeviceIdType.MESH


def split_two(x):
    hi = x.astype(BF16)
    lo = (x - hi.astype(F32)).astype(BF16)
    return jnp.concatenate([hi, lo], axis=1)


def kernel(
    x_hbm, live_hbm, gain_hbm, wq, wk, wv, wf, wl, we, ceil_hbm, resc_hbm, wo_hbm, mem_hbm, fade_hbm,
    out_ref, states,
    live_ref, xin, xrows, xs, gains, wcat, wall0, wall1, ceil, resc, fade, mem, packed,
    xg, acc, cs, cr, summed, ms, mg, xw, x1s, xr1, fin,
    load_sem, swap_send, swap_recv, a_send, a_recv, c_send, c_recv, e_send, e_recv, f_send, f_recv,
    w_send, w_recv, l_send, l_recv, far_sem,
):
    t = lax.axis_index("tp")
    d = lax.axis_index("dp")
    z = d // 2
    c = d % 2
    other = 1 - c
    away = (t + NZ - z) % NZ
    past_half = away // 9
    slot_here = (1 - past_half) * (2 * away - (away + 15) // 16) + past_half * (32 - 2 * away)

    load_rows = pltpu.make_async_copy(x_hbm, xin, load_sem.at[0])
    load_rows.start()
    barrier = pltpu.get_barrier_semaphore()

    y = t // SIDE
    x = t % SIDE

    def in_plane(up, right):
        return ((y + up) % SIDE) * SIDE + (x + right) % SIDE

    def greet_column(r, carry):
        for to in ((z + r) % NZ, (z + NZ - r) % NZ):
            pl.semaphore_signal(barrier, inc=1, device_id=(t, to * 2 + c), device_id_type=MESH)
        return carry

    for r in range(NEAR, 0, -1):
        greet_column(r, 0)
    for up, right in AROUND:
        for core in range(2):
            pl.semaphore_signal(
                barrier, inc=1, device_id=(in_plane(up, right), z * 2 + core), device_id_type=MESH
            )
    pl.semaphore_signal(barrier, inc=1, device_id=(t, z * 2 + other), device_id_type=MESH)

    mine = pl.ds(pl.multiple_of(c * 128, 128), 128)
    weights = (wq, wk, wv, wf, wl, we)
    loads = [pltpu.make_async_copy(live_hbm, live_ref, load_sem.at[14])]
    for p, w in enumerate(weights):
        loads.append(
            pltpu.make_async_copy(w, wcat.at[:, mine, pl.ds(p * 128, 128)], load_sem.at[1 + p])
        )
    loads.append(pltpu.make_async_copy(wo_hbm.at[0], wall0.at[t, :, mine], load_sem.at[7]))
    loads.append(pltpu.make_async_copy(wo_hbm.at[1], wall1.at[t], load_sem.at[13]))
    loads.append(pltpu.make_async_copy(gain_hbm, gains.at[c], load_sem.at[8]))
    loads.append(pltpu.make_async_copy(ceil_hbm, ceil, load_sem.at[9]))
    loads.append(pltpu.make_async_copy(resc_hbm, resc, load_sem.at[10]))
    loads.append(pltpu.make_async_copy(mem_hbm, mem, load_sem.at[11]))
    loads.append(pltpu.make_async_copy(fade_hbm, fade, load_sem.at[12]))
    for copy in loads:
        copy.start()

    lane = lax.broadcasted_iota(jnp.int32, (8, 128), 1)
    low_half = lane < 64
    row_at = lax.broadcasted_iota(jnp.int32, (256, 128), 0)
    lane_at = lax.broadcasted_iota(jnp.int32, (256, 128), 1)
    ones_block = jnp.where((row_at % 128) // 64 == lane_at // 64, 1.0, 0.0).astype(BF16)
    own_row = lax.broadcasted_iota(jnp.int32, (64, 128), 0)
    own_lane = lax.broadcasted_iota(jnp.int32, (64, 128), 1)
    diagonal = (own_lane % 64) == own_row

    def head_sum(x):
        return jnp.dot(split_two(x), ones_block, preferred_element_type=F32)

    load_rows.wait()
    xrows[...] = jnp.zeros((16, 128), F32)
    xrows[0:12, :] = xin[...].astype(F32)
    first = xrows[0:8, :]
    second = xrows[6:14, :]
    xs[0] = first.astype(BF16)
    xs[1] = second.astype(BF16)
    pl.semaphore_wait(barrier, 2 * (TP - 1) + 1 + 2 * NEAR)

    def remote(src, dst, send, recv, to_t, to_z, to_c):
        return pltpu.make_async_remote_copy(
            src_ref=src, dst_ref=dst, send_sem=send, recv_sem=recv,
            device_id=(to_t, to_z * 2 + to_c), device_id_type=MESH,
        )

    def to_sibling(src, i):
        return remote(src, src, swap_send.at[i], swap_recv.at[i], t, z, other)

    def row_copy(to, core):
        return remote(
            xs.at[core], xg.at[c, slot_here], a_send, a_recv, to, z, core
        )

    for up, right in AROUND:
        row_copy(in_plane(up, right), 0).start()
        row_copy(in_plane(up, right), 1).start()
    row_copy(t, other).start()
    for to in ((z + NEAR) % NZ, (z + NZ - NEAR) % NZ):
        pl.semaphore_signal(far_sem, inc=1, device_id=(t, to * 2 + c), device_id_type=MESH)
    xg[c, slot_here] = xs[c]

    swaps = [
        to_sibling(gains.at[c], 0),
        to_sibling(wcat.at[0, mine, :], 1),
        to_sibling(wcat.at[1, mine, :], 2),
        to_sibling(wall0.at[:, :, mine], 3),
    ]
    for copy in loads[1:7] + loads[9:10]:
        copy.wait()
    swaps[0].start()
    swaps[1].start()
    for copy in loads[0:1] + loads[7:9] + loads[10:]:
        copy.wait()

    def exit_step(r, carry):
        mine_here = wall0.at[t, :, mine]
        remote(mine_here, mine_here, w_send.at[0], w_recv.at[0], (t + r) % TP, z, c).start()
        return carry

    def exit_step_last(r, carry):
        remote(wall1.at[t], wall1.at[t], w_send.at[1], w_recv.at[1], (t + r) % TP, z, c).start()
        return carry

    for b in range(2):
        for s in range(3):
            packed[b, s] = jnp.concatenate([mem[b, s, 0], mem[b, s, 1]], axis=1)

    fade_columns = jnp.transpose(jnp.concatenate([fade[0], fade[1], jnp.zeros((4, 6), F32)], axis=0))

    def all_of(ref, send, recv):
        return remote(ref, ref, send, recv, t, z, other)

    def column(start, first, last):
        if last == 8:
            start((z + 8) % NZ, 15, 15)

        def step(i, carry):
            dist = min(last, 7) - i
            start((z + dist) % NZ, 2 * dist - 1, 2 * dist)
            start((z + NZ - dist) % NZ, 2 * dist, 2 * dist - 1)
            return carry

        lax.fori_loop(0, min(last, 7) - first + 1, step, 0)

    def project(b, rows, lo, hi):
        count = (hi - lo) * 8
        gained = jnp.concatenate(
            [(rows[h] * gains[h, b : b + 1, :].astype(F32)).astype(BF16) for h in range(2)],
            axis=1,
        )
        squares = jnp.sum(rows[0] * rows[0] + rows[1] * rows[1], axis=1, keepdims=True)
        squares = jnp.broadcast_to(squares, (count, 128)).reshape(hi - lo, 8, 128)
        token_at = lax.broadcasted_iota(jnp.int32, (hi - lo, 8, 128), 1)
        place_at = lax.broadcasted_iota(jnp.int32, (hi - lo, 8, 128), 2) // 16
        line = jnp.sum(jnp.where(token_at == place_at, squares, 0.0), axis=1, keepdims=True)
        rounded = line.astype(BF16).astype(F32)
        acc[lo:hi, 36:40, :] = jnp.zeros((hi - lo, 4, 128), F32)
        acc[lo:hi, 36:37, :] = rounded
        acc[lo:hi, 37:38, :] = line - rounded
        for p in range(6):
            part = jnp.dot(
                gained, wcat[b, :, p * 128 : (p + 1) * 128], preferred_element_type=F32
            )
            acc[lo:hi, p * 6 : p * 6 + 6, :] = part.reshape(hi - lo, 8, 128)[:, 0:6]
        cs[b, lo:hi] = acc[lo:hi].astype(BF16)

    def send_partials(b, first, last):
        def start(to, here, there):
            remote(cs.at[b, here, 0:SENT], cr.at[b, z, 0:SENT], c_send.at[b], c_recv.at[b], t, to, c).start()

        column(start, first, last)

    groups = ((0, 3, 1, 1), (3, 7, 2, 3), (7, 11, 4, 5), (11, 15, 6, 7), (15, 16, 8, 8))
    for b in range(2):
        if b == 0:
            swaps[0].wait_recv()
            swaps[1].wait_recv()
            all_of(fin.at[0:31], a_send, a_recv).wait_recv()
            rows = [xg[h].astype(F32).reshape(128, 128) for h in range(2)]
            for lo, hi, first, last in ((7, 16, 4, 8), (0, 7, 1, 3)):
                project(0, [row[8 * lo : 8 * hi] for row in rows], lo, hi)
                if last == 8:
                    pl.semaphore_wait(far_sem, 2)
                send_partials(0, first, last)
            lax.fori_loop(1, TP, exit_step, 0)
        else:
            swaps[2].wait_recv()
            swaps[3].wait_recv()
            for g, (lo, hi, first, last) in enumerate(groups):
                count = (hi - lo) * 8
                all_of(xw.at[0:15, lo:hi], f_send.at[g], f_recv.at[g]).wait_recv()
                heads = jnp.concatenate(
                    [xw[i, lo:hi].astype(F32).reshape(count, 128).astype(BF16) for i in range(TP)],
                    axis=1,
                )
                mix = jnp.dot(
                    heads, wall0[...].reshape(WIDTH, 256), preferred_element_type=F32
                )
                rows = []
                for h in range(2):
                    before = xg[h, lo:hi].astype(F32).reshape(count, 128)
                    after = (before + mix[:, 128 * h : 128 * h + 128]).astype(BF16).astype(F32)
                    x1s[h, lo:hi] = after.reshape(hi - lo, 8, 128).astype(BF16)
                    rows.append(after)
                project(1, rows, lo, hi)
                send_partials(1, first, last)
            residual = remote(
                x1s.at[other, slot_here], xr1, l_send, l_recv, t, z, other
            )
            residual.start()
            lax.fori_loop(1, TP, exit_step_last, 0)
        own = cs[b, 0]
        cr[b, z] = own

        row8 = lax.broadcasted_iota(jnp.int32, (8, 128), 0)
        live8 = jnp.zeros((8, 128), jnp.int32)
        for s in range(3):
            live8 = jnp.where(row8 // 2 == s, live_ref[s], live8)
        live_rows = (row8 % 2) < live8
        fade8 = jnp.where(low_half[0:6], fade_columns[:, 2 * b : 2 * b + 1], fade_columns[:, 2 * b + 1 : 2 * b + 2])

        all_of(cr.at[b, 0:15, 0:SENT], c_send.at[b], c_recv.at[b]).wait_recv()
        summed[0:40, :] = jnp.sum(cr[b].astype(F32), axis=0)
        line = summed[36:37, :] + summed[37:38, :]
        token_squares = jnp.sum(
            jnp.where(row8[0:6] == lane[0:6] // 16, line, 0.0), axis=1, keepdims=True
        ) * (1.0 / 16.0)
        row_scale = lax.rsqrt(token_squares / D + NORM_EPS)
        read, key, value, decay_pre, rate_pre, gate_pre = [
            summed[p * 6 : p * 6 + 6, :] * row_scale for p in range(6)
        ]
        decay = jnp.exp(fade8 - ceil[b : b + 1, :] * jax.nn.sigmoid(decay_pre))
        rate = jax.nn.sigmoid(rate_pre)
        gate = jax.nn.sigmoid(gate_pre)
        removal = key * rate / (head_sum(key * key) + 1e-06)
        spread = head_sum(
            jnp.concatenate(
                [jnp.where(diagonal, value[i : i + 1, :], 0.0) for i in range(6)], axis=0
            )
        )
        memory = [packed[b, s] for s in range(3)]
        readouts = [None] * 6
        spreads = [None] * 6
        for j in range(2):
            removed = head_sum(
                jnp.concatenate(
                    [memory[s] * key[2 * s + j : 2 * s + j + 1, :] for s in range(3)], axis=0
                )
            )
            for s in range(3):
                i = 2 * s + j
                updated = (
                    memory[s] * decay[i : i + 1, :]
                    - removed[64 * s : 64 * s + 64] * removal[i : i + 1, :]
                    + spread[64 * i : 64 * i + 64] * key[i : i + 1, :]
                )
                memory[s] = jnp.where(j < live_ref[s], updated, memory[s])
            read_out = head_sum(
                jnp.concatenate(
                    [memory[s] * read[2 * s + j : 2 * s + j + 1, :] for s in range(3)], axis=0
                )
            )
            for s in range(3):
                here = read_out[64 * s : 64 * s + 64]
                here = here - jnp.sum(here, axis=0, keepdims=True) * (1.0 / 64.0)
                spreads[2 * s + j] = jnp.sum(here * here, axis=0, keepdims=True)
                readouts[2 * s + j] = jnp.sum(
                    jnp.where(diagonal, here, 0.0), axis=0, keepdims=True
                )
        variance = jnp.concatenate(spreads, axis=0) * (1.0 / 64.0)
        centered = jnp.concatenate(readouts, axis=0)
        normed = centered * lax.rsqrt(variance + GROUP_EPS) * resc[b : b + 1, :]
        mixed = jnp.where(live_rows[0:6], normed * gate, 0.0)
        ms[b] = jnp.concatenate([mixed, jnp.zeros((2, 128), F32)], axis=0).astype(BF16)

        if b == 0:
            for g in (4, 3, 2, 1, 0):
                lo, hi, first, last = groups[g]

                def start(to, here, there):
                    remote(
                        ms.at[0], mg.at[there], e_send.at[g], e_recv.at[g], t, to, c
                    ).start()

                column(start, first, last)
            mg[0] = ms[0]
            all_of(wall0.at[0:15, :, mine], w_send.at[0], w_recv.at[0]).wait_recv()
            swaps[3].start()
            swaps[2].start()
        else:
            def start_both(to, here, there):
                for core in range(2):
                    remote(
                        ms.at[1], fin.at[c * TP + t], e_send.at[5], e_recv.at[5], z, to, core
                    ).start()

            column(start_both, 1, 8)

            @pl.when(t == z)
            def _():
                remote(
                    ms.at[1], fin.at[c * TP + t], e_send.at[5], e_recv.at[5], z, z, other
                ).start()
                fin[c * TP + t] = ms[1]

            @pl.when(t != z)
            def _():
                for core in range(2):
                    remote(
                        ms.at[1], fin.at[c * TP + t], e_send.at[5], e_recv.at[5], z, z, core
                    ).start()

        for s in range(3):
            states[b, s, 0] = memory[s][:, 0:64]
            states[b, s, 1] = memory[s][:, 64:128]

        if b == 0:
            for g, (lo, hi, first, last) in enumerate(groups):
                arriving = mg.at[max(lo, 1) : hi]
                all_of(arriving, e_send.at[g], e_recv.at[g]).wait_recv()

                for up, right in AROUND:
                    remote(
                        mg.at[lo:hi], xw.at[t, lo:hi], f_send.at[g], f_recv.at[g],
                        in_plane(up, right), z, c,
                    ).start()
                xw[t, lo:hi] = mg[lo:hi]

    all_of(wall1.at[0:15], w_send.at[1], w_recv.at[1]).wait_recv()
    residual.wait_recv()

    @pl.when(t == z)
    def _():
        all_of(fin.at[0:31], e_send.at[5], e_recv.at[5]).wait_recv()

    @pl.when(t != z)
    def _():
        all_of(fin, e_send.at[5], e_recv.at[5]).wait_recv()

    heads = jnp.concatenate(
        [
            jnp.concatenate([fin[i].astype(F32), fin[TP + i].astype(F32)], axis=0).astype(BF16)
            for i in range(TP)
        ],
        axis=1,
    )
    mix = jnp.dot(heads, wall1[...].reshape(WIDTH, 128), preferred_element_type=F32)
    here_rows = x1s[c, slot_here].astype(F32)
    there_rows = xr1[...].astype(F32)
    core = jnp.full((8, 128), c, jnp.int32)
    xrows[0:6, :] = (jnp.where(core == 0, here_rows, there_rows) + mix[0:8])[0:6]
    xrows[6:12, :] = (jnp.where(core == 0, there_rows, here_rows) + mix[8:16])[0:6]
    out_ref[...] = xrows[0:12, :].astype(BF16)

    for copy in swaps:
        copy.wait_send()
    residual.wait_send()
    all_of(fin.at[0:31], a_send, a_recv).wait_send()
    all_of(wall0.at[0:15, :, mine], w_send.at[0], w_recv.at[0]).wait_send()
    all_of(wall1.at[0:15], w_send.at[1], w_recv.at[1]).wait_send()
    for b in range(2):
        all_of(cr.at[b, 0:15, 0:SENT], c_send.at[b], c_recv.at[b]).wait_send()
    for g, (lo, hi, first, last) in enumerate(groups):
        all_of(mg.at[max(lo, 1) : hi], e_send.at[g], e_recv.at[g]).wait_send()
        all_of(xw.at[0:15, lo:hi], f_send.at[g], f_recv.at[g]).wait_send()

    @pl.when(t == z)
    def _():
        all_of(fin.at[0:31], e_send.at[5], e_recv.at[5]).wait_send()

    @pl.when(t != z)
    def _():
        all_of(fin, e_send.at[5], e_recv.at[5]).wait_send()


def store_results(rows_ref, states_ref, rows_out, states_out, sem):
    copies = [
        pltpu.make_async_copy(states_ref, states_out, sem.at[0]),
        pltpu.make_async_copy(rows_ref, rows_out, sem.at[1]),
    ]
    for copy in copies:
        copy.start()
    for copy in copies:
        copy.wait()


def shards(*arrays):
    arrays = arrays[:13] + (jnp.transpose(arrays[13], (0, 2, 1)),)
    arrays = tuple(pltpu.with_memory_space_constraint(a, pltpu.HBM) for a in arrays)
    hbm = pl.BlockSpec(memory_space=pltpu.HBM)
    in_specs = [hbm] * 14
    dma = pltpu.SemaphoreType.DMA
    results = pl.pallas_call(
        kernel,
        out_shape=(
            pltpu.VMEM((12, 128), BF16),
            pltpu.VMEM((2, 3, 2, 64, 64), F32),
        ),
        in_specs=in_specs,
        out_specs=(pl.BlockSpec(memory_space=pltpu.VMEM),) * 2,
        scratch_shapes=[
            pltpu.SMEM((3,), jnp.int32),
            pltpu.VMEM((12, 128), BF16),
            pltpu.VMEM((16, 128), F32),
            pltpu.VMEM((2, 8, 128), BF16),
            pltpu.VMEM((2, 2, 128), BF16),
            pltpu.VMEM((2, 256, 768), BF16),
            pltpu.VMEM((16, 128, 256), BF16),
            pltpu.VMEM((16, 128, 128), BF16),
            pltpu.VMEM((2, 128), F32),
            pltpu.VMEM((2, 128), F32),
            pltpu.VMEM((2, 2, 6), F32),
            pltpu.VMEM((2, 3, 2, 64, 64), F32),
            pltpu.VMEM((2, 3, 64, 128), F32),
            pltpu.VMEM((2, 16, 8, 128), BF16),
            pltpu.VMEM((16, 40, 128), F32),
            pltpu.VMEM((2, 16, 40, 128), BF16),
            pltpu.VMEM((2, 16, 40, 128), BF16),
            pltpu.VMEM((40, 128), F32),
            pltpu.VMEM((2, 8, 128), BF16),
            pltpu.VMEM((16, 8, 128), BF16),
            pltpu.VMEM((16, 16, 8, 128), BF16),
            pltpu.VMEM((2, 16, 8, 128), BF16),
            pltpu.VMEM((8, 128), BF16),
            pltpu.VMEM((32, 8, 128), BF16),
            dma((15,)),
            dma((4,)),
            dma((4,)),
            dma,
            dma,
            dma((2,)),
            dma((2,)),
            dma((6,)),
            dma((6,)),
            dma((5,)),
            dma((5,)),
            dma((2,)),
            dma((2,)),
            dma,
            dma,
            pltpu.SemaphoreType.REGULAR,
        ],
        compiler_params=pltpu.CompilerParams(collective_id=0, has_side_effects=True, vmem_limit_bytes=24 * 1024 * 1024),
    )(*arrays)
    return pl.pallas_call(
        store_results,
        out_shape=(
            jax.ShapeDtypeStruct((12, 128), BF16),
            jax.ShapeDtypeStruct((2, 3, 2, 64, 64), F32),
        ),
        in_specs=[pl.BlockSpec(memory_space=pltpu.VMEM)] * 2,
        out_specs=(hbm, hbm),
        scratch_shapes=[dma((2,))],
        compiler_params=pltpu.CompilerParams(vmem_limit_bytes=1024 * 1024),
    )(*results)


def solution(mesh):
    in_specs = (
        P("tp", "dp"),
        P("dp"),
        P(None, "dp"),
        P(None, "dp", "tp"),
        P(None, "dp", "tp"),
        P(None, "dp", "tp"),
        P(None, "dp", "tp"),
        P(None, "dp", "tp"),
        P(None, "dp", "tp"),
        P(None, "tp"),
        P(None, "tp"),
        P(None, "tp", "dp"),
        P(None, "dp", "tp", None, None),
        P(None, "dp", "tp"),
    )
    out_specs = (P("tp", "dp"), P(None, "dp", "tp", None, None))
    return jax.shard_map(shards, mesh=mesh, in_specs=in_specs, out_specs=out_specs, check_vma=False)
```
